32 devices in a mesh: fs: 8 (over z, x), tp: 4 (over y, core).
Axes of the slice: x: 2, y: 2, z: 4, core: 2. Of those that a mesh axis runs over, the one named last changes fastest.
Arguments:
- tokens: bfloat16 [6144, 2048], P('fs', 'tp'), may hold values from -6 to 6
- ffn_one_gain: float32 [2048], replicated, may hold values from 0.1 to 1.9
- ffn_one_gate: bfloat16 [2048, 5632], P('fs', 'tp'), may hold values from -0.125 to 0.125
- ffn_one_up: bfloat16 [2048, 5632], P('fs', 'tp'), may hold values from -0.125 to 0.125
- ffn_one_down: bfloat16 [5632, 2048], P('tp', 'fs'), may hold values from -0.078125 to 0.078125
- mix_gain: float32 [2048], replicated, may hold values from 0.1 to 1.9
- conv_value: bfloat16 [2048, 1024], P('fs', 'tp'), may hold values from -0.125 to 0.125
- conv_gate: bfloat16 [2048, 1024], P('fs', 'tp'), may hold values from -0.125 to 0.125
- conv_kernel: float32 [31, 1024], P(None, 'tp'), may hold values from -15 to 15
- conv_ln_gain: float32 [1024], P('tp'), may hold values from 0.1 to 1.9
- conv_out: bfloat16 [1024, 2048], P('tp', 'fs'), may hold values from -0.1875 to 0.1875
- ffn_two_gain: float32 [2048], replicated, may hold values from 0.1 to 1.9
- ffn_two_gate: bfloat16 [2048, 5632], P('fs', 'tp'), may hold values from -0.125 to 0.125
- ffn_two_up: bfloat16 [2048, 5632], P('fs', 'tp'), may hold values from -0.125 to 0.125
- ffn_two_down: bfloat16 [5632, 2048], P('tp', 'fs'), may hold values from -0.078125 to 0.078125
Outputs:
- layer_out: bfloat16 [6144, 2048], P('fs', 'tp')
The draws below stay inside these ranges and needn't reach their ends.
All inputs are finite; a program needn't handle non-finite values.
Results may differ from the reference program's by a relative error of at most 0.017.
Values may be sent and summed in bfloat16 or wider, within the bound.
A program may use at most 128 MiB of HBM per device.

```python
import jax
import jax.numpy as jnp
from jax import lax

D = 2048
FF = 5632
CONV = 1024
KW = 31
TOK_DEV = 768
TOKENS = 6144
N_FS = 8
N_TP = 4


def draw_conv_kernel(key, part):
    first_key, second_key = jax.random.split(jax.random.fold_in(key, 7))
    base = jnp.clip(jax.random.normal(first_key, (KW, CONV), jnp.float32), -4.0, 4.0) / jnp.sqrt(jnp.float32(KW))
    position = jnp.arange(CONV, dtype=jnp.float32) / jnp.float32(max(CONV - 1, 1))
    rising = 3.0 ** position * jax.random.uniform(second_key, (CONV,), jnp.float32, 0.7, 1.4)
    return base * rising[None, :]


def shard_levels(key, extent, cuts, least, high):
    factor_of, own = 1.0, jax.random.fold_in(key, 6)
    for dim, shards_of in cuts:
        heights = jnp.exp(jax.random.uniform(jax.random.fold_in(own, dim), (shards_of,), jnp.float32, least / len(cuts), high / len(cuts)))
        factor_of = factor_of * jnp.repeat(heights, extent[dim] // shards_of).reshape([-1 if axis == dim else 1 for axis in range(len(extent))])
    return factor_of


def scatter_about(stream_key, dims, width, bound, shards=(), held_as=jnp.bfloat16):
    entries = jax.random.normal(stream_key, dims, jnp.float32) * width
    if len(shards) > 0:
        entries = shard_levels(stream_key, dims, shards, -0.22, 0.18) * entries
    return jnp.clip(entries, min=-bound, max=bound).astype(held_as)


def setup_inputs(seed: int = 0) -> dict:
    key_of = jax.random.split(jax.random.key(seed), 16)
    tokens = scatter_about(key_of[0], (TOKENS, D), 1.0, 6.0, ((0, 8), (1, 4)))
    ffn_one_gain = jnp.clip(1.0 + 0.18 * jax.random.normal(key_of[1], (D,), jnp.float32), 0.1, 1.9)
    ffn_one_gate = scatter_about(key_of[2], (D, FF), D ** -0.5, 0.125, ((0, 8), (1, 4)))
    ffn_one_up = scatter_about(key_of[3], (D, FF), D ** -0.5, 0.125, ((0, 8), (1, 4)))
    ffn_one_down = scatter_about(key_of[4], (FF, D), FF ** -0.5, 0.078125, ((0, 4), (1, 8)))
    mix_gain = jnp.clip(1.0 + 0.18 * jax.random.normal(key_of[5], (D,), jnp.float32), 0.1, 1.9)
    conv_value = scatter_about(key_of[6], (D, CONV), D ** -0.5, 0.125, ((0, 8), (1, 4)))
    conv_gate = scatter_about(key_of[7], (D, CONV), D ** -0.5, 0.125, ((0, 8), (1, 4)))
    conv_kernel = draw_conv_kernel(jax.random.fold_in(key_of[15], 71), 0)
    conv_ln_gain = jnp.clip(1.0 + 0.18 * jax.random.normal(key_of[9], (CONV,), jnp.float32), 0.1, 1.9)
    conv_out = scatter_about(key_of[10], (CONV, D), CONV ** -0.5, 0.1875, ((0, 4), (1, 8)))
    ffn_two_gain = jnp.clip(1.0 + 0.18 * jax.random.normal(key_of[11], (D,), jnp.float32), 0.1, 1.9)
    ffn_two_gate = scatter_about(key_of[12], (D, FF), D ** -0.5, 0.125, ((0, 8), (1, 4)))
    ffn_two_up = scatter_about(key_of[13], (D, FF), D ** -0.5, 0.125, ((0, 8), (1, 4)))
    ffn_two_down = scatter_about(key_of[14], (FF, D), FF ** -0.5, 0.078125, ((0, 4), (1, 8)))
    return dict(tokens=tokens, ffn_one_gain=ffn_one_gain, ffn_one_gate=ffn_one_gate, ffn_one_up=ffn_one_up, ffn_one_down=ffn_one_down, mix_gain=mix_gain, conv_value=conv_value, conv_gate=conv_gate, conv_kernel=conv_kernel, conv_ln_gain=conv_ln_gain, conv_out=conv_out, ffn_two_gain=ffn_two_gain, ffn_two_gate=ffn_two_gate, ffn_two_up=ffn_two_up, ffn_two_down=ffn_two_down)


def rms_rows(rows_in, gain_vec):
    values = rows_in.astype(jnp.float32)
    scaled = values * lax.rsqrt(lax.optimization_barrier(jnp.mean(values * values, axis=-1, keepdims=True)) + 1e-06) * gain_vec
    return scaled.astype(jnp.bfloat16)

def block_sum(hidden, weight, blocks):
    span_width = hidden.shape[1] // blocks
    summed = jnp.zeros((hidden.shape[0], weight.shape[1]), jnp.float32)
    for block_index in range(blocks):
        lower = block_index * span_width
        partial_value = jnp.dot(hidden[:, lower:lower + span_width], weight[lower:lower + span_width], preferred_element_type=jnp.float32).astype(jnp.bfloat16)
        summed = summed + lax.optimization_barrier(partial_value).astype(jnp.float32)
    return summed

def half_ffn(residual, gain_vec, w_gate, w_up, w_down):
    normed = rms_rows(residual, gain_vec)
    gate_pre = jnp.dot(normed, w_gate, preferred_element_type=jnp.float32)
    up_pre = jnp.dot(normed, w_up, preferred_element_type=jnp.float32)
    hidden = (jax.nn.silu(gate_pre) * up_pre).astype(jnp.bfloat16)
    summed = block_sum(hidden, w_down, N_TP)
    return (residual.astype(jnp.float32) + 0.5 * summed).astype(jnp.bfloat16)

def conv_module(residual, mix_gain, conv_value, conv_gate, conv_kernel, conv_ln_gain, conv_out):
    normed = rms_rows(residual, mix_gain)
    value_pre = jnp.dot(normed, conv_value, preferred_element_type=jnp.float32)
    gate_pre = jnp.dot(normed, conv_gate, preferred_element_type=jnp.float32)
    gated_lin = value_pre * jax.nn.sigmoid(gate_pre)
    sequences = gated_lin.reshape(N_FS, TOK_DEV, CONV)
    half_span = KW // 2
    convolved = lax.conv_general_dilated(sequences, conv_kernel[:, None, :], (1,), [(half_span, half_span)], dimension_numbers=('NWC', 'WIO', 'NWC'), feature_group_count=CONV, precision=lax.Precision.HIGHEST).reshape(N_FS * TOK_DEV, CONV)
    mean_val = lax.optimization_barrier(jnp.sum(convolved, axis=1, keepdims=True)) / CONV
    sq_mean = lax.optimization_barrier(jnp.sum(convolved * convolved, axis=1, keepdims=True)) / CONV
    varied = sq_mean - mean_val * mean_val
    active = jax.nn.silu((convolved - mean_val) * lax.rsqrt(varied + 1e-05) * conv_ln_gain).astype(jnp.bfloat16)
    summed = block_sum(active, conv_out, N_TP)
    return (residual.astype(jnp.float32) + summed).astype(jnp.bfloat16)

def reference(tokens, ffn_one_gain, ffn_one_gate, ffn_one_up, ffn_one_down, mix_gain, conv_value, conv_gate, conv_kernel, conv_ln_gain, conv_out, ffn_two_gain, ffn_two_gate, ffn_two_up, ffn_two_down):
    stream = half_ffn(tokens, ffn_one_gain, ffn_one_gate, ffn_one_up, ffn_one_down)
    stream = conv_module(stream, mix_gain, conv_value, conv_gate, conv_kernel, conv_ln_gain, conv_out)
    return half_ffn(stream, ffn_two_gain, ffn_two_gate, ffn_two_up, ffn_two_down)
```

```python
from functools import partial

import jax
import jax.numpy as jnp
from jax import lax
from jax.experimental import pallas as pl
from jax.experimental.pallas import tpu as pltpu
from jax.sharding import PartitionSpec as P

F32 = jnp.float32
BF16 = jnp.bfloat16
MESH = pl.DeviceIdType.MESH
NT = (((1,), (1,)), ((), ()))
PAD = 16


def split_fs(total):
    inner = 1
    while total % (inner * 2) == 0 and (inner * 2) ** 2 <= total:
        inner *= 2
    return total // inner, inner


class Plan:
    def __init__(self, fs, tp, tok, ws, cs, kernel_rows):
        self.fs, self.tp = fs, tp
        self.z, self.x = split_fs(fs)
        self.y = tp // 2
        self.rows, width = tok
        self.kb = ws[2]
        self.nb = width // self.kb
        self.ffh = ws[1] // 2
        self.ch = cs[0] // 3
        unit = 256 if self.ch % 256 == 0 else 128
        self.nw = unit
        self.ffp = -(-self.ffh // unit) * unit
        self.nc = self.ffp // unit
        self.lw = max(self.ffp, 3 * self.ch)
        self.half_rows = self.rows // 2
        self.cell = self.half_rows // self.y
        self.kw = kernel_rows
        self.dim = self.kb * fs


def body(g, *refs):
    (tok, ws, cs, gains, ck, cg, out) = refs[:7]
    (LW, XF, XR, ACC, HID, PP, RA, RB, RC, GB, SB, SR, AB) = refs[7:20]
    (s_loc, s_tok, zs, zr, xs, xr, ags, agr, as_, ar, bs, br, cs_s, cr, gys, gyr, gzs, gzr, gcs, gcr, sts, st_r, os_, orr) = refs[20:]
    Z, X, Y, TP, FS = g.z, g.x, g.y, g.tp, g.fs
    rows, kb, nb, ffh, ch = g.rows, g.kb, g.nb, g.ffh, g.ch
    TH, R = g.half_rows, g.cell
    fs_i, tp_i = lax.axis_index("fs"), lax.axis_index("tp")
    z, x = fs_i // X, fs_i % X
    y, core = tp_i // 2, tp_i % 2
    zp = z % 2
    oq = 1 - zp
    zb = z - zp
    zmate = zb + oq
    fs_mate = zmate * X + x
    tp_core = y * 2 + 1 - core

    def zx(j):
        if isinstance(j, int):
            hi, lo = j - j % 2, j % 2
        else:
            hi, lo = j - lax.rem(j, 2), lax.rem(j, 2)
        return xor2(zb, hi) + lo

    def xor2(a, b):
        r, bit = 0, 2
        while bit < Z:
            abit = lax.rem(a // bit, 2)
            bbit = (b // bit) % 2 if isinstance(b, int) else lax.rem(b // bit, 2)
            r = r + bit * lax.rem(abit + bbit, 2)
            bit *= 2
        return r

    def xor_z(k):
        r, bit = 0, 1
        while bit < Z:
            r = r + bit * lax.rem(lax.rem(z // bit, 2) + (k // bit) % 2, 2)
            bit *= 2
        return r

    def s_of(i):
        if isinstance(i, int):
            return zx(i // X) * X + lax.rem(x + i % X, X)
        return zx(i // X) * X + lax.rem(x + lax.rem(i, X), X)

    def rcopy(src, dst, ssem, rsem, fs_to, tp_to):
        return pltpu.make_async_remote_copy(
            src_ref=src, dst_ref=dst, send_sem=ssem, recv_sem=rsem,
            device_id=(fs_to, tp_to), device_id_type=MESH,
        )

    def yo(dy):
        return lax.rem(y + dy, Y)

    bar = pltpu.get_barrier_semaphore()
    peers = [(xor_z(k) * X + x, tp_i) for k in range(1, Z)]
    peers += [(z * X + lax.rem(x + dx, X), tp_i) for dx in range(1, X)]
    peers += [(fs_i, lax.rem(tp_i + dt, TP)) for dt in range(1, TP)]
    for f_to, t_to in peers:
        pl.semaphore_signal(bar, inc=1, device_id=(f_to, t_to), device_id_type=MESH)

    def local_weight(p):
        if p == 3:
            return pltpu.make_async_copy(cs, LW.at[3, fs_i, pl.ds(0, 3 * ch)], s_loc.at[p])
        src = ws.at[p if p < 3 else p - 1, pl.ds(pl.multiple_of(zp * ffh, 16), ffh)]
        return pltpu.make_async_copy(src, LW.at[p, fs_i, pl.ds(0, ffh)], s_loc.at[p])

    def local_tok(b):
        return pltpu.make_async_copy(
            tok.at[:, pl.ds(b * kb, kb)], XF.at[zp, tp_i * nb + b], s_tok.at[b]
        )

    for b in range(nb):
        local_tok(b).start()
    for p in range(7):
        local_weight(p).start()
    pl.semaphore_wait(bar, len(peers))

    def zsend(p, k):
        to = xor_z(k)
        if p == 3:
            src, dst = cs, LW.at[3, fs_i, pl.ds(0, 3 * ch)]
        else:
            src = ws.at[p if p < 3 else p - 1, pl.ds(pl.multiple_of(lax.rem(to, 2) * ffh, 16), ffh)]
            dst = LW.at[p, fs_i, pl.ds(0, ffh)]
        return rcopy(src, dst, zs.at[p, k], zr.at[p, k], to * X + x, tp_i)

    def xsend(p, j, dx):
        s = zx(j) * X + x
        ref = LW.at[p, s, pl.ds(0, 3 * ch if p == 3 else ffh)]
        return rcopy(ref, ref, xs.at[p, j, dx], xr.at[p, s], z * X + lax.rem(x + dx, X), tp_i)

    def xwait(p, s):
        ref = LW.at[p, s, pl.ds(0, 3 * ch if p == 3 else ffh)]
        rcopy(ref, ref, xs.at[p, 0, 1 % X], xr.at[p, s], z * X + x, tp_i).wait_recv()

    def start_zsend(m):
        p, k = m // (Z - 1), m % (Z - 1) + 1
        if p < 7:
            zsend(p, k).start()

    AHEAD = Z + 1

    def k_of(j):
        return jnp.where(zp == 0, j, j + 1 - 2 * (j % 2))

    def advance(n):
        if n >= 7 * Z:
            return
        p, j = n // Z, n % Z
        if j:
            start_zsend(p * (Z - 1) + j - 1 + AHEAD)

        if j < 2:
            @pl.when(zp == j)
            def _():
                local_weight(p).wait()

            @pl.when(zp != j)
            def _():
                zsend(p, 1).wait_recv()
        else:
            rcopy(LW.at[p, fs_i, pl.ds(0, 3 * ch if p == 3 else ffh)], LW.at[p, fs_i, pl.ds(0, 3 * ch if p == 3 else ffh)],
                  zs.at[p, 1], zr.at[p, k_of(j)], fs_i, tp_i).wait_recv()
        for dx in range(1, X):
            xsend(p, j, dx).start()

    def ag_piece(q, t):
        return XF.at[q, pl.ds(t * nb, nb)]

    def agz():
        r = ag_piece(zp, tp_i)
        return rcopy(r, r, ags.at[0], agr.at[0], fs_mate, tp_i)

    def agy(q, qi, dy):
        r = ag_piece(q, tp_i)
        return rcopy(r, r, ags.at[1 + qi * Y + dy], agr.at[1 + qi * Y + dy], fs_i, yo(dy) * 2 + core)

    def agy_wait(q, qi, dy):
        agy(q, qi, dy).wait_recv()

    def agc(q, qi, dy):
        r = ag_piece(q, lax.rem(y + Y - dy, Y) * 2 + core)
        n = 1 + 2 * Y + qi * Y + dy
        return rcopy(r, r, ags.at[n], agr.at[n], fs_i, tp_core)

    for b in range(nb):
        local_tok(b).wait()
    agz().start()
    for dy in range(1, Y):
        agy(zp, 0, dy).start()
    agc(zp, 0, 0).start()
    for m in range(AHEAD):
        start_zsend(m)
    if g.lw > ffh:
        def zero(i, c):
            for p in (0, 1, 2, 4, 5, 6):
                LW[p, i, ffh:] = jnp.zeros((g.lw - ffh, kb), BF16)
            return c
        lax.fori_loop(0, FS, zero, 0)
    GB[0:PAD] = jnp.zeros((PAD, ch), F32)
    GB[PAD + rows:] = jnp.zeros((PAD, ch), F32)
    advance(0)
    agz().wait_recv()
    for dy in range(1, Y):
        agy(oq, 1, dy).start()
    agc(oq, 1, 0).start()
    advance(1)
    for dy in range(1, Y):
        agy_wait(zp, 0, dy)
        agc(zp, 0, dy).start()
    advance(2)
    for dy in range(1, Y):
        agy_wait(oq, 1, dy)
        agc(oq, 1, dy).start()
    for n in range(3, Z):
        advance(n)
    for dy in range(Y):
        agc(zp, 0, dy).wait_recv()
        agc(oq, 1, dy).wait_recv()
    agz().wait_send()
    for dy in range(Y):
        agc(zp, 0, dy).wait_send()
        agc(oq, 1, dy).wait_send()
        if dy:
            agy(zp, 0, dy).wait_send()
            agy(oq, 1, dy).wait_send()

    my_cell = pl.multiple_of(core * TH + y * R, 16)

    def cell_of(yy):
        return pl.multiple_of(core * TH + yy * R, 16)

    def keep(s, c):
        XR[s] = XF[zp, s, pl.ds(my_cell, R)]
        return c

    lax.fori_loop(0, FS, keep, 0)

    NR = 64

    def normalize(q, layer):
        def chunk(c, carry):
            at = pl.ds(pl.multiple_of(c * NR, NR), NR)
            total = jnp.zeros((NR, kb), F32)
            for s in range(FS):
                v = XF[q, s, at].astype(F32)
                total = total + v * v
            scale = lax.rsqrt(jnp.sum(total, axis=1, keepdims=True) / g.dim + 1e-06)
            for s in range(FS):
                XF[q, s, at] = (XF[q, s, at].astype(F32) * scale * gains[layer, s]).astype(BF16)
            return carry
        lax.fori_loop(0, rows // NR, chunk, 0)

    def up_piece(p, half, j):
        def each(e, c):
            s = zx(j) * X + lax.rem(x + e, X)

            @pl.when(e > 0)
            def _():
                xwait(p, s)

            def seq(t, c2):
                q, n = t // g.nc, lax.rem(t, g.nc)
                w = LW[p, s, pl.ds(pl.multiple_of(n * g.nw, g.nw), g.nw)]
                d = lax.dot_general(XF[q, s], w, NT, preferred_element_type=F32)
                if j == 0:
                    @pl.when(e == 0)
                    def _():
                        ACC[half, q, n] = d

                    @pl.when(e > 0)
                    def _():
                        ACC[half, q, n] += d
                else:
                    ACC[half, q, n] += d
                return c2
            lax.fori_loop(0, 2 * g.nc, seq, 0)
            return c
        lax.fori_loop(0, X, each, 0)

    def a_copy(s, nq):
        at = pl.ds(pl.multiple_of((1 - core) * TH, 16), TH)
        here = pl.ds(0, TH)
        return rcopy(PP.at[s, pl.ds(0, nq), at], RA.at[s, pl.ds(0, nq), here], as_.at[s], ar.at[s], fs_i, tp_core)

    def b_copy(s, nq, dy):
        return rcopy(PP.at[s, pl.ds(0, nq), pl.ds(cell_of(yo(dy)), R)], RB.at[dy - 1, s, pl.ds(0, nq)],
                     bs.at[s, dy], br.at[s, dy], fs_i, yo(dy) * 2 + core)

    def c_copy(s):
        return rcopy(PP.at[s, oq, pl.ds(my_cell, R)], RC.at[s], cs_s.at[s], cr.at[s], fs_mate, tp_i)

    def stage_b(s, nq):
        a_copy(s, nq).wait_recv()
        mine = pl.ds(pl.multiple_of(core * TH, 16), TH)
        for q in range(nq):
            PP[s, q, mine] = (PP[s, q, mine].astype(F32) + RA[s, q].astype(F32)).astype(BF16)
        for dy in range(1, Y):
            b_copy(s, nq, dy).start()

    def b_sum(s, q):
        total = PP[s, q, pl.ds(my_cell, R)].astype(F32)
        for dy in range(1, Y):
            total = total + RB[dy - 1, s, q].astype(F32)
        return total

    def stage_c(s):
        for dy in range(1, Y):
            b_copy(s, 2, dy).wait_recv()
        PP[s, oq, pl.ds(my_cell, R)] = b_sum(s, oq).astype(BF16)
        c_copy(s).start()

    def ffn_sum(s):
        c_copy(s).wait_recv()
        total = b_sum(s, zp) + RC[s].astype(F32)
        return (XR[s].astype(F32) + 0.5 * total).astype(BF16)

    def gy_copy(q, qi, s, dy, yy):
        r = XF.at[q, s, pl.ds(cell_of(yy), R)]
        return rcopy(r, r, gys.at[qi, s, dy], gyr.at[qi, s, dy], fs_i, yo(dy) * 2 + core)

    def gz_copy(s):
        r = XF.at[zp, s, pl.ds(my_cell, R)]
        return rcopy(r, r, gzs.at[s], gzr.at[s], fs_mate, tp_i)

    def gc_copy(q, qi):
        r = XF.at[q, :, pl.ds(pl.multiple_of(core * TH, 16), TH)]
        return rcopy(r, r, gcs.at[qi], gcr.at[qi], fs_i, tp_core)

    def loop(n, f):
        def step(i, c):
            f(i)
            return c
        lax.fori_loop(0, n, step, 0)

    def half_step(p0, n0, finish, fill):
        n = n0
        for half in range(2):
            for j in range(Z):
                while n < (p0 + half) * Z + j + 2:
                    advance(n)
                    n += 1
                up_piece(p0 + half, half, j)

        def act(t):
            q = t // (rows // NR)
            at = pl.ds(pl.multiple_of(lax.rem(t, rows // NR) * NR, NR), NR)
            for c in range(g.nc):
                gate = ACC[0, q, c, at]
                HID[q, at, c * g.nw:(c + 1) * g.nw] = (gate * jax.nn.sigmoid(gate) * ACC[1, q, c, at]).astype(BF16)
        loop(2 * (rows // NR), act)

        for j in range(Z):
            while n < (p0 + 2) * Z + j + 2:
                advance(n)
                n += 1

            def each(e):
                i = j * X + e
                s = s_of(i)

                @pl.when(e > 0)
                def _():
                    xwait(p0 + 2, s)

                def seq(q):
                    PP[s, q] = jnp.dot(HID[q], LW[p0 + 2, s, pl.ds(0, g.ffp)], preferred_element_type=F32).astype(BF16)
                loop(2, seq)
                a_copy(s, 2).start()

                @pl.when(i >= 1)
                def _():
                    stage_b(s_of(i - 1), 2)

                @pl.when(i >= 2)
                def _():
                    stage_c(s_of(i - 2))

                @pl.when(i >= 3)
                def _():
                    finish(s_of(i - 3))
            loop(X, each)
        stage_b(s_of(FS - 1), 2)
        stage_c(s_of(FS - 2))
        finish(s_of(FS - 3))
        fill(n)
        stage_c(s_of(FS - 1))
        finish(s_of(FS - 2))
        finish(s_of(FS - 1))

    def sends_done(s):
        a_copy(s, 2).wait_send()
        c_copy(s).wait_send()
        for dy in range(1, Y):
            b_copy(s, 2, dy).wait_send()

    normalize(0, 0)
    normalize(1, 0)

    def finish_one(s):
        v = ffn_sum(s)
        XR[s] = v
        XF[zp, s, pl.ds(my_cell, R)] = v
        for dy in range(1, Y):
            gy_copy(zp, 0, s, dy, y).start()

    def fill_one(n):
        for k in range(n, 4 * Z):
            advance(k)

    half_step(0, Z, finish_one, fill_one)
    n = 4 * Z

    def own_arrived(s):
        for dy in range(1, Y):
            gy_copy(zp, 0, s, dy, y).wait_recv()
    loop(FS, own_arrived)
    gc_copy(zp, 0).start()
    loop(FS, sends_done)

    def own_sent(s):
        for dy in range(1, Y):
            gy_copy(zp, 0, s, dy, y).wait_send()
    loop(FS, own_sent)
    gc_copy(zp, 0).wait()

    normalize(zp, 1)

    def mix(i):
        e = lax.rem(i, X)
        s = s_of(i)

        @pl.when(e > 0)
        def _():
            xwait(3, s)
        for part in range(2):
            d = lax.dot_general(XF[zp, s], LW[3, s, part * ch:(part + 1) * ch], NT, preferred_element_type=F32)

            @pl.when(i == 0)
            def _():
                ACC[part, 0, 0] = d

            @pl.when(i > 0)
            def _():
                ACC[part, 0, 0] += d
    loop(FS, mix)

    def gated(t):
        at = pl.multiple_of(t * NR, NR)
        gate = ACC[1, 0, 0, pl.ds(at, NR)]
        GB[pl.ds(pl.multiple_of(at + PAD, 16), NR)] = ACC[0, 0, 0, pl.ds(at, NR)] * jax.nn.sigmoid(gate)
    loop(rows // NR, gated)

    off = PAD - g.kw // 2
    lanes = 128

    def taps(t):
        at = pl.multiple_of(t * NR, NR)
        sum_one = jnp.zeros((NR, 1), F32)
        sum_two = jnp.zeros((NR, 1), F32)
        for c in range(ch // lanes):
            cols = slice(c * lanes, (c + 1) * lanes)
            window = GB[pl.ds(at, NR + 2 * PAD), cols]
            total = jnp.zeros((NR, lanes), F32)
            for k in range(g.kw):
                total = total + ck[k:k + 1, cols] * window[k + off:k + off + NR]
            ACC[0, 1, 0, pl.ds(at, NR), cols] = total
            sum_one = sum_one + jnp.sum(total, axis=1, keepdims=True)
            sum_two = sum_two + jnp.sum(total * total, axis=1, keepdims=True)
        which = lax.broadcasted_iota(jnp.int32, (NR, 128), 1)
        AB[pl.ds(at, NR)] = jnp.where(which == 0, sum_one, jnp.where(which == 1, sum_two, 0.0))
    loop(rows // NR, taps)

    def flip(t):
        at = pl.ds(pl.multiple_of(t * 128, 128), 128)
        SB[:, at] = AB[at].T[0:8]
    loop(rows // 128, flip)

    def st_copy(dt):
        return rcopy(SB, SR.at[dt - 1], sts.at[dt], st_r.at[dt], fs_i, lax.rem(tp_i + dt, TP))

    for dt in range(1, TP):
        st_copy(dt).start()
    advance(n)
    n += 1
    for dt in range(1, TP):
        st_copy(dt).wait()

    def unflip(t):
        at = pl.ds(pl.multiple_of(t * 128, 128), 128)
        total = SB[:, at]
        for dt in range(1, TP):
            total = total + SR[dt - 1, :, at]
        AB[at] = jnp.concatenate([total, jnp.zeros((120, 128), F32)], axis=0).T
    loop(rows // 128, unflip)

    def activate(t):
        at = pl.ds(pl.multiple_of(t * NR, NR), NR)
        stats = AB[at]
        mean = stats[:, 0:1] / (ch * TP)
        var = stats[:, 1:2] / (ch * TP) - mean * mean
        v = (ACC[0, 1, 0, at] - mean) * lax.rsqrt(var + 1e-05) * cg[...]
        HID[0, at, 0:ch] = (v * jax.nn.sigmoid(v)).astype(BF16)
    loop(rows // NR, activate)

    def mixed(s):
        b_total = b_sum(s, 0)
        v = (XR[s].astype(F32) + b_total).astype(BF16)
        XR[s] = v
        XF[zp, s, pl.ds(my_cell, R)] = v
        gz_copy(s).start()
        for dy in range(1, Y):
            gy_copy(zp, 0, s, dy, y).start()

    def mixed_block(s):
        for dy in range(1, Y):
            b_copy(s, 1, dy).wait_recv()
        mixed(s)

    def pass_on(s):
        gz_copy(s).wait_recv()
        for dy in range(1, Y):
            gy_copy(oq, 1, s, dy, y).start()

    def project(i):
        s = s_of(i)
        PP[s, 0] = jnp.dot(HID[0, :, 0:ch], LW[3, s, 2 * ch:3 * ch], preferred_element_type=F32).astype(BF16)
        a_copy(s, 1).start()

        @pl.when(i >= 1)
        def _():
            stage_b(s_of(i - 1), 1)
    loop(FS, project)
    stage_b(s_of(FS - 1), 1)
    for i in range(FS + 2):
        if i < FS:
            mixed_block(s_of(i))
        if i >= 2:
            pass_on(s_of(i - 2))
        if i % 2 == 1 and n < 6 * Z:
            advance(n)
            n += 1

    def all_arrived(s):
        for dy in range(1, Y):
            gy_copy(zp, 0, s, dy, y).wait_recv()
    loop(FS, all_arrived)
    gc_copy(zp, 0).start()

    def rest_arrived(s):
        for dy in range(1, Y):
            gy_copy(oq, 1, s, dy, y).wait_recv()
    loop(FS, rest_arrived)
    gc_copy(oq, 1).start()

    def mix_sends(s):
        a_copy(s, 1).wait_send()
        gz_copy(s).wait_send()
        for dy in range(1, Y):
            b_copy(s, 1, dy).wait_send()
            gy_copy(zp, 0, s, dy, y).wait_send()
            gy_copy(oq, 1, s, dy, y).wait_send()
    loop(FS, mix_sends)
    gc_copy(zp, 0).wait()
    gc_copy(oq, 1).wait()

    normalize(0, 2)
    normalize(1, 2)

    def o_copy(s, slot):
        owner = s // nb
        b = lax.rem(s, nb)
        return rcopy(XR.at[s], out.at[b, pl.ds(my_cell, R)], os_.at[s], orr.at[b, slot], fs_i, owner)

    def finish_two(s):
        v = ffn_sum(s)
        owner = s // nb
        XR[s] = v

        @pl.when(owner == tp_i)
        def _():
            out[lax.rem(s, nb), pl.ds(my_cell, R)] = v

        @pl.when(owner != tp_i)
        def _():
            o_copy(s, lax.rem(tp_i - owner + TP, TP)).start()

    def fill_two(n):
        pass

    half_step(4, n, finish_two, fill_two)

    for b in range(nb):
        for slot in range(1, TP):
            rcopy(XR.at[0], out.at[b, pl.ds(0, R)], os_.at[0], orr.at[b, slot], fs_i, tp_i).wait_recv()

    def out_sent(s):
        @pl.when(s // nb != tp_i)
        def _():
            o_copy(s, 0).wait_send()
    loop(FS, out_sent)
    loop(FS, sends_done)
    for p in range(7):
        for k in range(1, Z):
            zsend(p, k).wait_send()
        for j in range(Z):
            for dx in range(1, X):
                xsend(p, j, dx).wait_send()


def per_device(fs, tp, tokens, g0, wg0, wu0, wd0, g1, cv, cgate, ck, cln, co, g2, wg1, wu1, wd1):
    ws = jnp.stack([wg0.T, wu0.T, wd0, wg1.T, wu1.T, wd1])
    cs = jnp.concatenate([cv.T, cgate.T, co], axis=0)
    g = Plan(fs, tp, tokens.shape, ws.shape, cs.shape, ck.shape[0])
    gains = jnp.stack([g0, g1, g2]).reshape(3, fs, 1, g.kb)
    Z, X, Y, TP, FS = g.z, g.x, g.y, g.tp, g.fs
    dma = pltpu.SemaphoreType.DMA
    vm = pltpu.VMEM
    scratch = [
        vm((7, FS, g.lw, g.kb), BF16),
        vm((2, FS, g.rows, g.kb), BF16),
        vm((FS, g.cell, g.kb), BF16),
        vm((2, 2, g.nc, g.rows, g.nw), F32),
        vm((2, g.rows, g.ffp), BF16),
        vm((FS, 2, g.rows, g.kb), BF16),
        vm((FS, 2, g.half_rows, g.kb), BF16),
        vm((Y - 1, FS, 2, g.cell, g.kb), BF16),
        vm((FS, g.cell, g.kb), BF16),
        vm((g.rows + 2 * PAD, g.ch), F32),
        vm((8, g.rows), F32),
        vm((TP - 1, 8, g.rows), F32),
        vm((g.rows, 128), F32),
        dma((7,)), dma((g.nb,)),
        dma((7, Z)), dma((7, Z)),
        dma((7, Z, X)), dma((7, FS)),
        dma((1 + 4 * Y,)), dma((1 + 4 * Y,)),
        dma((FS,)), dma((FS,)),
        dma((FS, Y)), dma((FS, Y)),
        dma((FS,)), dma((FS,)),
        dma((2, FS, Y)), dma((2, FS, Y)),
        dma((FS,)), dma((FS,)),
        dma((2,)), dma((2,)),
        dma((TP,)), dma((TP,)),
        dma((FS,)), dma((g.nb, TP)),
    ]
    anyspace = pl.BlockSpec(memory_space=pl.ANY)
    vmem = pl.BlockSpec(memory_space=pltpu.VMEM)
    res = pl.pallas_call(
        partial(body, g),
        out_shape=jax.ShapeDtypeStruct((g.nb, g.rows, g.kb), BF16),
        in_specs=[anyspace, anyspace, anyspace, vmem, vmem, vmem],
        out_specs=vmem,
        scratch_shapes=scratch,
        compiler_params=pltpu.CompilerParams(
            collective_id=0, has_side_effects=True, vmem_limit_bytes=67043328
        ),
        name="layer",
    )(tokens, ws, cs, gains, ck, cln.reshape(1, -1))
    return res.transpose(1, 0, 2).reshape(g.rows, g.nb * g.kb)


def solution(mesh):
    fs, tp = mesh.shape["fs"], mesh.shape["tp"]
    both = P("fs", "tp")
    down = P("tp", "fs")
    in_specs = (both, P(), both, both, down, P(), both, both, P(None, "tp"), P("tp"), down, P(), both, both, down)
    return jax.shard_map(
        partial(per_device, fs, tp), mesh=mesh, in_specs=in_specs, out_specs=both, check_vma=False
    )
```

```python
from functools import partial

import jax
import jax.numpy as jnp
from jax import lax
from jax.experimental import pallas as pl
from jax.experimental.pallas import tpu as pltpu
from jax.sharding import PartitionSpec as P

F32 = jnp.float32
BF16 = jnp.bfloat16
MESH = pl.DeviceIdType.MESH
NT = (((1,), (1,)), ((), ()))
PAD = 16


def split_fs(total):
    inner = 1
    while total % (inner * 2) == 0 and (inner * 2) ** 2 <= total:
        inner *= 2
    return total // inner, inner


class Plan:
    def __init__(self, fs, tp, tok, ws, co, kernel_rows):
        self.fs, self.tp = fs, tp
        self.z, self.x = split_fs(fs)
        self.y = tp // 2
        self.rows, width = tok
        self.kb = ws[1]
        self.nb = width // self.kb
        self.ffh = ws[0] // 2
        self.ch = co[0]
        unit = 256 if self.ch % 256 == 0 else 128
        self.ffp = -(-self.ffh // unit) * unit
        self.lw = max(self.ffp, 3 * self.ch)
        self.half_rows = self.rows // 2
        self.cell = self.half_rows // self.y
        self.kw = kernel_rows
        self.dim = self.kb * fs


class Marks:
    def __init__(self):
        self.open = None

    def __call__(self, name):
        if self.open is not None:
            self.open.__exit__(None, None, None)
        self.open = None
        if name is not None:
            self.open = jax.named_scope(name)
            self.open.__enter__()


def body(g, *refs):
    mark = Marks()
    mark("entry")
    (tok, *ws, cv, cgate, co, ga, gb, gc, ck, cg, out) = refs[:16]
    (LW, XF, XR, ACC, HID, PP, RA, RB, RC, RD, RE, RF, GB, CV, SB, SR, AB) = refs[16:33]
    gains = (ga, gb, gc)
    (s_loc, s_conv, s_tok, zs, zr, xs, xr, ags, agr, as_, ar, bs, br, cs_s, cr, ds, dr, es, er, fss, fr, gys, gyr, gzs, gzr, gcs, gcr, sts, st_r, os_, orr) = refs[33:]
    Z, X, Y, TP, FS = g.z, g.x, g.y, g.tp, g.fs
    rows, kb, nb, ffh, ch = g.rows, g.kb, g.nb, g.ffh, g.ch
    TH, R = g.half_rows, g.cell
    fs_i, tp_i = lax.axis_index("fs"), lax.axis_index("tp")
    z, x = fs_i // X, fs_i % X
    y, core = tp_i // 2, tp_i % 2
    zp = z % 2
    oq = 1 - zp
    zb = z - zp
    zmate = zb + oq
    fs_mate = zmate * X + x
    tp_core = y * 2 + 1 - core

    def zx(j):
        if isinstance(j, int):
            hi, lo = j - j % 2, j % 2
        else:
            hi, lo = j - lax.rem(j, 2), lax.rem(j, 2)
        return xor2(zb, hi) + lo

    def xor2(a, b):
        r, bit = 0, 2
        while bit < Z:
            abit = lax.rem(a // bit, 2)
            bbit = (b // bit) % 2 if isinstance(b, int) else lax.rem(b // bit, 2)
            r = r + bit * lax.rem(abit + bbit, 2)
            bit *= 2
        return r

    def xor_z(k):
        r, bit = 0, 1
        while bit < Z:
            r = r + bit * lax.rem(lax.rem(z // bit, 2) + (k // bit) % 2, 2)
            bit *= 2
        return r

    def s_of(i):
        if isinstance(i, int):
            return zx(i // X) * X + lax.rem(x + i % X, X)
        return zx(i // X) * X + lax.rem(x + lax.rem(i, X), X)

    def rcopy(src, dst, ssem, rsem, fs_to, tp_to):
        return pltpu.make_async_remote_copy(
            src_ref=src, dst_ref=dst, send_sem=ssem, recv_sem=rsem,
            device_id=(fs_to, tp_to), device_id_type=MESH,
        )

    def yo(dy):
        return lax.rem(y + dy, Y)

    bar = pltpu.get_barrier_semaphore()
    peers = [(xor_z(k) * X + x, tp_i) for k in range(1, Z)]
    peers += [(z * X + lax.rem(x + dx, X), tp_i) for dx in range(1, X)]
    peers += [(fs_i, lax.rem(tp_i + dt, TP)) for dt in range(1, TP)]
    for f_to, t_to in peers:
        pl.semaphore_signal(bar, inc=1, device_id=(f_to, t_to), device_id_type=MESH)

    def local_weight(p):
        if p == 3:
            return pltpu.make_async_copy(co, LW.at[3, fs_i, pl.ds(2 * ch, ch)], s_loc.at[p])
        src = ws[p if p < 3 else p - 1].at[pl.ds(pl.multiple_of(zp * ffh, 16), ffh)]
        return pltpu.make_async_copy(src, LW.at[p, fs_i, pl.ds(0, ffh)], s_loc.at[p])

    def local_tok(b):
        return pltpu.make_async_copy(
            tok.at[:, pl.ds(b * kb, kb)], XF.at[zp, tp_i * nb + b], s_tok.at[b]
        )

    for b in range(nb):
        local_tok(b).start()
    for p in range(7):
        local_weight(p).start()

    def local_conv(n):
        return pltpu.make_async_copy((cv, cgate)[n], HID.at[n, pl.ds(0, kb), pl.ds(0, ch)], s_conv.at[n])

    for n in range(2):
        local_conv(n).start()
    pl.semaphore_wait(bar, len(peers))

    def zsend(p, k):
        to = xor_z(k)
        if p == 3:
            src = dst = LW.at[3, fs_i, pl.ds(0, 3 * ch)]
        else:
            src = ws[p if p < 3 else p - 1].at[pl.ds(pl.multiple_of(lax.rem(to, 2) * ffh, 16), ffh)]
            dst = LW.at[p, fs_i, pl.ds(0, ffh)]
        return rcopy(src, dst, zs.at[p, k], zr.at[p, k], to * X + x, tp_i)

    def xsend(p, k, dx):
        s = (xor_z(k) if k else z) * X + x
        ref = LW.at[p, s, pl.ds(0, 3 * ch if p == 3 else ffh)]
        return rcopy(ref, ref, xs.at[p, k, dx], xr.at[p, s], z * X + lax.rem(x + dx, X), tp_i)

    def xwait(p, s):
        ref = LW.at[p, s, pl.ds(0, 3 * ch if p == 3 else ffh)]
        rcopy(ref, ref, xs.at[p, 0, 1 % X], xr.at[p, s], z * X + x, tp_i).wait_recv()

    inner = jnp.logical_and(z > 0, z < Z - 1)
    by_end = jnp.logical_or(z == 1, z == Z - 2)

    def relay(p):
        ref = LW.at[p, fs_mate, pl.ds(0, 3 * ch if p == 3 else ffh)]
        return rcopy(ref, ref, zs.at[p, 0], zr.at[p, Z - 1], xor_z(Z - 2) * X + x, tp_i)

    def near(p):
        zsend(p, 1).start()

    def near_two(p):
        @pl.when(jnp.logical_not(inner))
        def _():
            for k in range(2, Z - 1):
                zsend(p, k).start()

    def far(p, ks=tuple(range(2, Z))):
        @pl.when(inner)
        def _():
            for k in ks:
                zsend(p, k).start()

    hooks = {
        0: lambda: near(1),
        1: lambda: near_two(1),
        Z - 1: lambda: near(2),
        Z: lambda: near_two(2),
    }

    def own(p):
        if p < 7:
            if p != 3:
                local_weight(p).wait()
            for dx in range(1, X):
                xsend(p, 0, dx).start()

    done = [0]

    def advance(p, k):
        last = min(p, 6) * (Z - 1) + (k if p < 7 else Z - 1)
        while done[0] < last:
            m = done[0]
            q, d = m // (Z - 1), m % (Z - 1) + 1
            zsend(q, d).wait_recv()
            if d == 1:
                @pl.when(by_end)
                def _():
                    relay(q).start()
                if q < 6:
                    far(q + 1)
            if m in hooks:
                hooks[m]()
            for dx in range(1, X):
                xsend(q, d, dx).start()
            if m % (Z - 1) == Z - 2 and q >= 2:
                own(q + 1)
            done[0] = m + 1

    def ag_piece(q, t):
        return XF.at[q, pl.ds(t * nb, nb)]

    def agz():
        r = ag_piece(zp, tp_i)
        return rcopy(r, r, ags.at[0], agr.at[0], fs_mate, tp_i)

    def agy(q, qi, dy):
        r = ag_piece(q, tp_i)
        return rcopy(r, r, ags.at[1 + qi * Y + dy], agr.at[1 + qi * Y + dy], fs_i, yo(dy) * 2 + core)

    def agy_wait(q, qi, dy):
        agy(q, qi, dy).wait_recv()

    def agc(q, qi, dy):
        r = ag_piece(q, lax.rem(y + Y - dy, Y) * 2 + core)
        n = 1 + 2 * Y + qi * Y + dy
        return rcopy(r, r, ags.at[n], agr.at[n], fs_i, tp_core)

    mark("tok")
    for b in range(nb):
        local_tok(b).wait()
    agz().start()
    for dy in range(1, Y):
        agy(zp, 0, dy).start()
    agc(zp, 0, 0).start()
    near(0)
    near_two(0)
    far(0, tuple(range(3, Z)))
    for p in range(3):
        own(p)
    for n in range(2):
        local_conv(n).wait()
        LW[3, fs_i, n * ch:(n + 1) * ch] = HID[n, 0:kb, 0:ch].T
    local_weight(3).wait()
    if g.lw > ffh:
        def zero(i, c):
            for p in (0, 1, 2, 4, 5, 6):
                LW[p, i, ffh:] = jnp.zeros((g.lw - ffh, kb), BF16)
            return c
        lax.fori_loop(0, FS, zero, 0)
    GB[0:PAD] = jnp.zeros((PAD, ch), F32)
    GB[PAD + rows:] = jnp.zeros((PAD, ch), F32)
    mark("agz")
    agz().wait_recv()
    for dy in range(1, Y):
        agy(oq, 1, dy).start()
    agc(oq, 1, 0).start()
    far(0, (2,))
    mark("agy0")
    for dy in range(1, Y):
        agy_wait(zp, 0, dy)
        agc(zp, 0, dy).start()
    mark("adv01")
    advance(0, 1)
    mark("agy1")
    for dy in range(1, Y):
        agy_wait(oq, 1, dy)
        agc(oq, 1, dy).start()
    mark("adv03")
    advance(0, 2)
    mark("agc")
    for dy in range(Y):
        agc(zp, 0, dy).wait_recv()
        agc(oq, 1, dy).wait_recv()
    agz().wait_send()
    for dy in range(Y):
        agc(zp, 0, dy).wait_send()
        agc(oq, 1, dy).wait_send()
        if dy:
            agy(zp, 0, dy).wait_send()
            agy(oq, 1, dy).wait_send()

    my_cell = pl.multiple_of(core * TH + y * R, 16)

    def cell_of(yy):
        return pl.multiple_of(core * TH + yy * R, 16)

    mine = pl.ds(pl.multiple_of(core * TH, 16), TH)

    def keep(s, c):
        XR[s] = XF[zp, s, mine]
        return c

    lax.fori_loop(0, FS, keep, 0)

    NR = 64

    def normalize(q, layer):
        def chunk(c, carry):
            at = pl.ds(pl.multiple_of(c * NR, NR), NR)
            total = jnp.zeros((NR, kb), F32)
            for s in range(FS):
                v = XF[q, s, at].astype(F32)
                total = total + v * v
            scale = lax.rsqrt(jnp.sum(total, axis=1, keepdims=True) / g.dim + 1e-06)
            for s in range(FS):
                XF[q, s, at] = (XF[q, s, at].astype(F32) * scale * gains[layer][s]).astype(BF16)
            return carry
        lax.fori_loop(0, rows // NR, chunk, 0)

    MR = rows // 2

    def arrived(p):
        def one(i):
            @pl.when(lax.rem(i, X) > 0)
            def _():
                xwait(p, s_of(i))
        loop(FS, one)

    def features(p, q, at, width):
        total = None
        for s in range(FS):
            d = lax.dot_general(XF[q, s, at], LW[p, s, 0:width], NT, preferred_element_type=F32)
            total = d if total is None else total + d
        return total

    def chunks(n, f):
        def one(t):
            f(t // (rows // MR), pl.ds(pl.multiple_of(lax.rem(t, rows // MR) * MR, MR), MR))
        loop(n * (rows // MR), one)

    def loop(n, f):
        def step(i, c):
            f(i)
            return c
        lax.fori_loop(0, n, step, 0)

    def a_copy(s, nq):
        at = pl.ds(pl.multiple_of((1 - core) * TH, 16), TH)
        here = pl.ds(0, TH)
        return rcopy(PP.at[s, pl.ds(0, nq), at], RA.at[s, pl.ds(0, nq), here], as_.at[s], ar.at[s], fs_i, tp_core)

    def b_copy(s, dy):
        return rcopy(PP.at[s, :, pl.ds(cell_of(yo(dy)), R)], RB.at[dy - 1, s],
                     bs.at[s, dy], br.at[s, dy], fs_i, yo(dy) * 2 + core)

    def c_copy(s):
        return rcopy(PP.at[s, oq, pl.ds(my_cell, R)], RC.at[s], cs_s.at[s], cr.at[s], fs_mate, tp_i)

    def d_copy(s, dy):
        return rcopy(PP.at[s, 0, mine], RD.at[dy - 1, s], ds.at[s, dy], dr.at[s, dy], fs_i, yo(dy) * 2 + core)

    def stage_a(s, nq):
        a_copy(s, nq).wait_recv()
        for q in range(nq):
            PP[s, q, mine] = (PP[s, q, mine].astype(F32) + RA[s, q].astype(F32)).astype(BF16)

    def e_copy(s):
        return rcopy(PP.at[s, oq, mine], RE.at[s], es.at[s], er.at[s], fs_mate, tp_i)

    def f_copy(s, dy):
        return rcopy(PP.at[s, zp, pl.ds(cell_of(yo(dy)), R)], RF.at[dy - 1, s],
                     fss.at[s, dy], fr.at[s, dy], fs_i, yo(dy) * 2 + core)

    def by_parity(i, first, second):
        if isinstance(i, int):
            (second if i % 2 else first)()
        else:
            pl.when(lax.rem(i, 2) == 0)(first)
            pl.when(lax.rem(i, 2) == 1)(second)

    def stage_one(i):
        s = s_of(i)
        stage_a(s, 2)

        def even():
            for dy in range(1, Y):
                b_copy(s, dy).start()

        def odd():
            e_copy(s).start()
        by_parity(i, even, odd)

    def b_sum(s, q):
        total = PP[s, q, pl.ds(my_cell, R)].astype(F32)
        for dy in range(1, Y):
            total = total + RB[dy - 1, s, q].astype(F32)
        return total

    def stage_two(i):
        s = s_of(i)

        def even():
            for dy in range(1, Y):
                b_copy(s, dy).wait_recv()
            PP[s, oq, pl.ds(my_cell, R)] = b_sum(s, oq).astype(BF16)
            c_copy(s).start()

        def odd():
            e_copy(s).wait_recv()
            PP[s, zp, mine] = (PP[s, zp, mine].astype(F32) + RE[s].astype(F32)).astype(BF16)
            for dy in range(1, Y):
                f_copy(s, dy).start()
        by_parity(i, even, odd)

    def residual(s, total):
        return (XR[s, pl.ds(pl.multiple_of(y * R, 16), R)].astype(F32) + 0.5 * total).astype(BF16)

    def stage_three(i, put):
        s = s_of(i)

        def even():
            c_copy(s).wait_recv()
            put(s, residual(s, b_sum(s, zp) + RC[s].astype(F32)))

        def odd():
            total = PP[s, zp, pl.ds(my_cell, R)].astype(F32)
            for dy in range(1, Y):
                f_copy(s, dy).wait_recv()
                total = total + RF[dy - 1, s].astype(F32)
            put(s, residual(s, total))
        by_parity(i, even, odd)
        return s

    def sends_done(i):
        s = s_of(i)
        a_copy(s, 2).wait_send()

        def even():
            c_copy(s).wait_send()
            for dy in range(1, Y):
                b_copy(s, dy).wait_send()

        def odd():
            e_copy(s).wait_send()
            for dy in range(1, Y):
                f_copy(s, dy).wait_send()
        by_parity(i, even, odd)

    def gy_copy(q, qi, s, dy):
        r = XF.at[q, s, pl.ds(my_cell, R)]
        return rcopy(r, r, gys.at[s, dy], gyr.at[s, dy], fs_i, yo(dy) * 2 + core)

    def gc_copy(q, qi, s, dy, at):
        r = XF.at[q, s, at]
        return rcopy(r, r, gcs.at[qi, s, dy], gcr.at[qi, s, dy], fs_i, tp_core)

    def cell_from(dy):
        return pl.ds(cell_of(lax.rem(y - dy + Y, Y)), R)

    def plane_copy(s, at):
        r = XF.at[zp, s, at]
        return rcopy(r, r, gzs.at[s], gzr.at[s], fs_mate, tp_i)

    LAG_TWO, LAG_THREE = 3, 5

    def half_step(p0, before_down, plan, finish, after):
        mark(f"adv_p{p0}")
        advance(p0, Z - 1)
        advance(p0 + 1, 1)
        mark(f"wait_p{p0}")
        arrived(p0)
        mark(f"adv2_p{p0}")
        advance(p0 + 1, 2)
        mark(f"gate_p{p0}")

        def gate(q, at):
            ACC[q, at] = features(p0, q, at, g.ffp)
        chunks(2, gate)
        mark(f"adv_p{p0 + 1}")
        advance(p0 + 1, Z - 1)
        advance(p0 + 2, 1)
        mark(f"wait_p{p0 + 1}")
        arrived(p0 + 1)
        mark(f"up_p{p0 + 1}")

        def up(q, at):
            v = ACC[q, at]
            HID[q, at] = (v * jax.nn.sigmoid(v) * features(p0 + 1, q, at, g.ffp)).astype(BF16)
        chunks(2, up)

        before_down()
        for j in range(Z):
            mark(f"adv_p{p0 + 2}_{j}")
            plan[j]()

            def each(e):
                i = j * X + e
                s = s_of(i)

                @pl.when(e > 0)
                def _():
                    xwait(p0 + 2, s)

                def seq(q):
                    PP[s, q] = jnp.dot(HID[q], LW[p0 + 2, s, pl.ds(0, g.ffp)], preferred_element_type=F32).astype(BF16)
                loop(2, seq)
                a_copy(s, 2).start()

                @pl.when(i >= 1)
                def _():
                    stage_one(i - 1)

                @pl.when(i >= LAG_TWO)
                def _():
                    stage_two(i - LAG_TWO)

                @pl.when(i >= LAG_THREE)
                def _():
                    finish(i - LAG_THREE)
            mark(f"down_p{p0 + 2}_{j}")
            loop(X, each)
        mark("drain_a")
        stage_one(FS - 1)
        mark("drain_b")
        for i in range(FS - LAG_TWO, FS):
            stage_two(i)
            if i >= LAG_THREE - LAG_TWO:
                finish(i + LAG_TWO - LAG_THREE)
        mark("fill")
        after()
        mark("drain_c")
        for i in range(FS + LAG_TWO - LAG_THREE, FS):
            finish(i)

    mark("norm0")
    normalize(0, 0)
    normalize(1, 0)

    def put_one(s, v):
        XF[zp, s, pl.ds(my_cell, R)] = v

    def finish_one(i):
        s = stage_three(i, put_one)
        for dy in range(1, Y):
            gy_copy(zp, 0, s, dy).start()
        gc_copy(zp, 0, s, 0, pl.ds(my_cell, R)).start()

    def after_one():
        near(4)
        near_two(4)
        advance(3, Z - 1)

    half_step(
        0,
        lambda: near(3),
        [lambda: advance(2, 1), lambda: advance(2, 2), lambda: (near_two(3), advance(2, Z - 1)), lambda: advance(3, 1)],
        finish_one,
        after_one,
    )

    mark("own_arr")

    def from_y(s):
        for dy in range(1, Y):
            gy_copy(zp, 0, s, dy).wait_recv()
            gc_copy(zp, 0, s, dy, cell_from(dy)).start()
        XR[s] = XF[zp, s, mine]
    loop(FS, from_y)
    mark("own_core")
    near(5)
    loop(FS, sends_done)

    def one_sends(s):
        for dy in range(Y):
            if dy:
                gy_copy(zp, 0, s, dy).wait_send()
            gc_copy(zp, 0, s, dy, pl.ds(my_cell, R)).wait()
    loop(FS, one_sends)

    mark("adv41")
    advance(4, 1)
    mark("norm1")
    normalize(zp, 1)
    mark("mix")

    arrived(3)

    def mix(q, at):
        both = features(3, zp, at, 2 * ch)
        GB[pl.ds(pl.multiple_of(at.start + PAD, 16), MR)] = both[:, :ch] * jax.nn.sigmoid(both[:, ch:])
    chunks(1, mix)

    off = PAD - g.kw // 2
    lanes = 128

    def taps(t):
        at = pl.multiple_of(t * NR, NR)
        sum_one = jnp.zeros((NR, 1), F32)
        sum_two = jnp.zeros((NR, 1), F32)
        for c in range(ch // lanes):
            cols = slice(c * lanes, (c + 1) * lanes)
            window = GB[pl.ds(at, NR + 2 * PAD), cols]
            total = jnp.zeros((NR, lanes), F32)
            for r in range(8):
                taps_here = [k for k in range(g.kw) if (k + off) % 8 == r]
                shifted = window[r:max(taps_here) + off + NR]
                for k in taps_here:
                    total = total + ck[k:k + 1, cols] * shifted[k + off - r:k + off - r + NR]
            CV[pl.ds(at, NR), cols] = total
            sum_one = sum_one + jnp.sum(total, axis=1, keepdims=True)
            sum_two = sum_two + jnp.sum(total * total, axis=1, keepdims=True)
        which = lax.broadcasted_iota(jnp.int32, (NR, 128), 1)
        AB[pl.ds(at, NR)] = jnp.where(which == 0, sum_one, jnp.where(which == 1, sum_two, 0.0))
    mark("taps")
    loop(rows // NR, taps)
    mark("stats")

    def flip(t):
        at = pl.ds(pl.multiple_of(t * 128, 128), 128)
        SB[:, at] = AB[at].T[0:8]
    loop(rows // 128, flip)

    def st_copy(dt):
        return rcopy(SB, SR.at[dt - 1], sts.at[dt], st_r.at[dt], fs_i, lax.rem(tp_i + dt, TP))

    for dt in range(1, TP):
        st_copy(dt).start()
    near_two(5)
    advance(4, 2)
    for dt in range(1, TP):
        st_copy(dt).wait()

    def unflip(t):
        at = pl.ds(pl.multiple_of(t * 128, 128), 128)
        total = SB[:, at]
        for dt in range(1, TP):
            total = total + SR[dt - 1, :, at]
        AB[at] = jnp.concatenate([total, jnp.zeros((120, 128), F32)], axis=0).T
    loop(rows // 128, unflip)

    def activate(t):
        at = pl.ds(pl.multiple_of(t * NR, NR), NR)
        stats = AB[at]
        mean = stats[:, 0:1] / (ch * TP)
        var = stats[:, 1:2] / (ch * TP) - mean * mean
        v = (CV[at] - mean) * lax.rsqrt(var + 1e-05) * cg[...]
        HID[0, at, 0:ch] = (v * jax.nn.sigmoid(v)).astype(BF16)
    mark("active")
    loop(rows // NR, activate)

    def y_total(s):
        for dy in range(1, Y):
            d_copy(s, dy).wait_recv()
        own_part = PP[s, 0, mine].astype(F32)
        if Y == 2:
            return own_part + RD[0, s].astype(F32)
        total = jnp.zeros((TH, kb), F32)
        for yy in range(Y):
            slot = lax.rem(y - yy + Y, Y)
            term = RD[lax.max(slot - 1, 0), s].astype(F32)
            total = total + jnp.where(slot == 0, own_part, term)
        return total

    def mixed(i):
        s = s_of(i)
        v = (XR[s].astype(F32) + y_total(s)).astype(BF16)
        XR[s] = v
        XF[zp, s, mine] = v
        plane_copy(s, mine).start()
        gc_copy(zp, 0, s, 0, mine).start()

    def pass_on(i):
        s = s_of(i)
        plane_copy(s, mine).wait_recv()
        gc_copy(oq, 1, s, 0, mine).start()

    mark("project")

    def project(i):
        s = s_of(i)
        PP[s, 0] = jnp.dot(HID[0, :, 0:ch], LW[3, s, 2 * ch:3 * ch], preferred_element_type=F32).astype(BF16)
        a_copy(s, 1).start()

        @pl.when(i >= 1)
        def _():
            prev = s_of(i - 1)
            stage_a(prev, 1)
            for dy in range(1, Y):
                d_copy(prev, dy).start()
    loop(FS, project)
    last = s_of(FS - 1)
    stage_a(last, 1)
    for dy in range(1, Y):
        d_copy(last, dy).start()
    LAG_ON = 5
    for i in range(FS + LAG_ON):
        mark(f"mixed_{i}")
        if i < FS:
            mixed(i)
        if i == FS - 1:
            near(6)
            near_two(6)
        if i >= LAG_ON:
            pass_on(i - LAG_ON)
        if i % 2 == 1 and i < 2 * Z:
            mark(f"mixadv_{i}")
            advance(4 + (i // 2 + 2) // (Z - 1), (i // 2 + 2) % (Z - 1) + 1)
    mark("mixsends")

    def mix_sends(s):
        a_copy(s, 1).wait_send()
        plane_copy(s, mine).wait_send()
        gc_copy(zp, 0, s, 0, mine).wait()
        gc_copy(oq, 1, s, 0, mine).wait()
        for dy in range(1, Y):
            d_copy(s, dy).wait_send()
    loop(FS, mix_sends)

    mark("norm2")
    normalize(0, 2)
    normalize(1, 2)

    def o_copy(s, slot):
        owner = s // nb
        b = lax.rem(s, nb)
        return rcopy(XR.at[s, 0:R], out.at[pl.ds(my_cell, R), pl.ds(pl.multiple_of(b * kb, kb), kb)], os_.at[s], orr.at[b, slot], fs_i, owner)

    def put_two(s, v):
        XR[s, 0:R] = v

    def finish_two(i):
        s = stage_three(i, put_two)
        owner = s // nb

        @pl.when(owner == tp_i)
        def _():
            out[pl.ds(my_cell, R), pl.ds(pl.multiple_of(lax.rem(s, nb) * kb, kb), kb)] = XR[s, 0:R]

        @pl.when(owner != tp_i)
        def _():
            o_copy(s, lax.rem(tp_i - owner + TP, TP)).start()

    half_step(4, lambda: None, [partial(advance, 6, min(j + 1, Z - 1)) for j in range(Z)], finish_two, lambda: None)

    mark("out_wait")
    for b in range(nb):
        for slot in range(1, TP):
            rcopy(XR.at[0, 0:R], out.at[pl.ds(0, R), pl.ds(b * kb, kb)], os_.at[0], orr.at[b, slot], fs_i, tp_i).wait_recv()

    mark("end_sends")

    def out_sent(s):
        @pl.when(s // nb != tp_i)
        def _():
            o_copy(s, 0).wait_send()
    loop(FS, out_sent)

    loop(FS, sends_done)
    for p in range(7):
        for k in range(1, Z - 1):
            zsend(p, k).wait_send()

        @pl.when(inner)
        def _():
            zsend(p, Z - 1).wait_send()

        @pl.when(by_end)
        def _():
            relay(p).wait_send()
        for k in range(Z):
            for dx in range(1, X):
                xsend(p, k, dx).wait_send()
    mark(None)


def per_device(fs, tp, tokens, g0, wg0, wu0, wd0, g1, cv, cgate, ck, cln, co, g2, wg1, wu1, wd1):
    ws = [wg0.T, wu0.T, wd0, wg1.T, wu1.T, wd1]
    g = Plan(fs, tp, tokens.shape, wd0.shape, co.shape, ck.shape[0])
    gains = [v.reshape(fs, 1, g.kb) for v in (g0, g1, g2)]
    Z, X, Y, TP, FS = g.z, g.x, g.y, g.tp, g.fs
    dma = pltpu.SemaphoreType.DMA
    vm = pltpu.VMEM
    scratch = [
        vm((7, FS, g.lw, g.kb), BF16),
        vm((2, FS, g.rows, g.kb), BF16),
        vm((FS, g.half_rows, g.kb), BF16),
        vm((2, g.rows, g.ffp), F32),
        vm((2, g.rows, g.ffp), BF16),
        vm((FS, 2, g.rows, g.kb), BF16),
        vm((FS, 2, g.half_rows, g.kb), BF16),
        vm((Y - 1, FS, 2, g.cell, g.kb), BF16),
        vm((FS, g.cell, g.kb), BF16),
        vm((Y - 1, FS, g.half_rows, g.kb), BF16),
        vm((FS, g.half_rows, g.kb), BF16),
        vm((Y - 1, FS, g.cell, g.kb), BF16),
        vm((g.rows + 2 * PAD, g.ch), F32),
        vm((g.rows, g.ch), F32),
        vm((8, g.rows), F32),
        vm((TP - 1, 8, g.rows), F32),
        vm((g.rows, 128), F32),
        dma((7,)), dma((2,)), dma((g.nb,)),
        dma((7, Z)), dma((7, Z)),
        dma((7, Z, X)), dma((7, FS)),
        dma((1 + 4 * Y,)), dma((1 + 4 * Y,)),
        dma((FS,)), dma((FS,)),
        dma((FS, Y)), dma((FS, Y)),
        dma((FS,)), dma((FS,)),
        dma((FS, Y)), dma((FS, Y)),
        dma((FS,)), dma((FS,)),
        dma((FS, Y)), dma((FS, Y)),
        dma((FS, Y)), dma((FS, Y)),
        dma((FS,)), dma((FS,)),
        dma((2, FS, Y)), dma((2, FS, Y)),
        dma((TP,)), dma((TP,)),
        dma((FS,)), dma((g.nb, TP)),
    ]
    anyspace = pl.BlockSpec(memory_space=pl.ANY)
    vmem = pl.BlockSpec(memory_space=pltpu.VMEM)
    res = pl.pallas_call(
        partial(body, g),
        out_shape=jax.ShapeDtypeStruct((g.rows, g.nb * g.kb), BF16),
        in_specs=[anyspace] * 10 + [vmem] * 5,
        out_specs=vmem,
        scratch_shapes=scratch,
        compiler_params=pltpu.CompilerParams(
            collective_id=0, has_side_effects=True, vmem_limit_bytes=67043328
        ),
        name="layer",
    )(tokens, *ws, cv, cgate, co, *gains, ck, cln.reshape(1, -1))
    return res


def solution(mesh):
    fs, tp = mesh.shape["fs"], mesh.shape["tp"]
    both = P("fs", "tp")
    down = P("tp", "fs")
    in_specs = (both, P(), both, both, down, P(), both, both, P(None, "tp"), P("tp"), down, P(), both, both, down)
    return jax.shard_map(
        partial(per_device, fs, tp), mesh=mesh, in_specs=in_specs, out_specs=both, check_vma=False
    )
```

```python
from functools import partial

import jax
import jax.numpy as jnp
from jax import lax
from jax.experimental import pallas as pl
from jax.experimental.pallas import tpu as pltpu
from jax.sharding import PartitionSpec as P

F32 = jnp.float32
BF16 = jnp.bfloat16
MESH = pl.DeviceIdType.MESH
NT = (((1,), (1,)), ((), ()))
PAD = 16


def split_fs(total):
    inner = 1
    while total % (inner * 2) == 0 and (inner * 2) ** 2 <= total:
        inner *= 2
    return total // inner, inner


class Plan:
    def __init__(self, fs, tp, tok, ws, co, kernel_rows):
        self.fs, self.tp = fs, tp
        self.z, self.x = split_fs(fs)
        self.y = tp // 2
        self.rows, width = tok
        self.kb = ws[1]
        self.nb = width // self.kb
        self.ffh = ws[0] // 2
        self.ch = co[0]
        unit = 256 if self.ch % 256 == 0 else 128
        self.ffp = -(-self.ffh // unit) * unit
        self.lw = max(self.ffp, 3 * self.ch)
        self.half_rows = self.rows // 2
        self.cell = self.half_rows // self.y
        self.kw = kernel_rows
        self.dim = self.kb * fs


class Marks:
    def __init__(self):
        self.open = None

    def __call__(self, name):
        if self.open is not None:
            self.open.__exit__(None, None, None)
        self.open = None
        if name is not None:
            self.open = jax.named_scope(name)
            self.open.__enter__()


def body(g, *refs):
    mark = Marks()
    mark("entry")
    (tok, *ws, cv, cgate, co, ga, gb, gc, ck, cg, out) = refs[:16]
    (LW, XF, XR, ACC, HID, PP, RA, RB, RC, RD, RE, RF, GB, CV, SB, SR, AB) = refs[16:33]
    gains = (ga, gb, gc)
    (s_loc, s_conv, s_tok, zs, zr, xs, xr, ags, agr, as_, ar, bs, br, cs_s, cr, ds, dr, es, er, fss, fr, gys, gyr, gzs, gzr, gcs, gcr, sts, st_r, os_, orr) = refs[33:]
    Z, X, Y, TP, FS = g.z, g.x, g.y, g.tp, g.fs
    rows, kb, nb, ffh, ch = g.rows, g.kb, g.nb, g.ffh, g.ch
    TH, R = g.half_rows, g.cell
    fs_i, tp_i = lax.axis_index("fs"), lax.axis_index("tp")
    z, x = fs_i // X, fs_i % X
    y, core = tp_i // 2, tp_i % 2
    zp = z % 2
    oq = 1 - zp
    zb = z - zp
    zmate = zb + oq
    fs_mate = zmate * X + x
    tp_core = y * 2 + 1 - core

    def zx(j):
        if isinstance(j, int):
            hi, lo = j - j % 2, j % 2
        else:
            hi, lo = j - lax.rem(j, 2), lax.rem(j, 2)
        return xor2(zb, hi) + lo

    def xor2(a, b):
        r, bit = 0, 2
        while bit < Z:
            abit = lax.rem(a // bit, 2)
            bbit = (b // bit) % 2 if isinstance(b, int) else lax.rem(b // bit, 2)
            r = r + bit * lax.rem(abit + bbit, 2)
            bit *= 2
        return r

    def xor_z(k):
        r, bit = 0, 1
        while bit < Z:
            r = r + bit * lax.rem(lax.rem(z // bit, 2) + (k // bit) % 2, 2)
            bit *= 2
        return r

    def s_of(i):
        if isinstance(i, int):
            return zx(i // X) * X + lax.rem(x + i % X, X)
        return zx(i // X) * X + lax.rem(x + lax.rem(i, X), X)

    def rcopy(src, dst, ssem, rsem, fs_to, tp_to):
        return pltpu.make_async_remote_copy(
            src_ref=src, dst_ref=dst, send_sem=ssem, recv_sem=rsem,
            device_id=(fs_to, tp_to), device_id_type=MESH,
        )

    def yo(dy):
        return lax.rem(y + dy, Y)

    bar = pltpu.get_barrier_semaphore()
    peers = [(xor_z(k) * X + x, tp_i) for k in range(1, Z)]
    peers += [(z * X + lax.rem(x + dx, X), tp_i) for dx in range(1, X)]
    peers += [(fs_i, lax.rem(tp_i + dt, TP)) for dt in range(1, TP)]
    for f_to, t_to in peers:
        pl.semaphore_signal(bar, inc=1, device_id=(f_to, t_to), device_id_type=MESH)

    def local_weight(p):
        if p == 3:
            return pltpu.make_async_copy(co, LW.at[3, fs_i, pl.ds(2 * ch, ch)], s_loc.at[p])
        src = ws[p if p < 3 else p - 1].at[pl.ds(pl.multiple_of(zp * ffh, 16), ffh)]
        return pltpu.make_async_copy(src, LW.at[p, fs_i, pl.ds(0, ffh)], s_loc.at[p])

    def local_tok(b):
        return pltpu.make_async_copy(
            tok.at[:, pl.ds(b * kb, kb)], XF.at[zp, tp_i * nb + b], s_tok.at[b]
        )

    for b in range(nb):
        local_tok(b).start()
    for p in range(7):
        local_weight(p).start()

    def local_conv(n):
        return pltpu.make_async_copy((cv, cgate)[n], HID.at[n, pl.ds(0, kb), pl.ds(0, ch)], s_conv.at[n])

    for n in range(2):
        local_conv(n).start()
    pl.semaphore_wait(bar, len(peers))

    def zsend(p, k):
        to = xor_z(k)
        if p == 3:
            src = dst = LW.at[3, fs_i, pl.ds(0, 3 * ch)]
        else:
            src = ws[p if p < 3 else p - 1].at[pl.ds(pl.multiple_of(lax.rem(to, 2) * ffh, 16), ffh)]
            dst = LW.at[p, fs_i, pl.ds(0, ffh)]
        return rcopy(src, dst, zs.at[p, k], zr.at[p, k], to * X + x, tp_i)

    def xsend(p, k, dx):
        s = (xor_z(k) if k else z) * X + x
        ref = LW.at[p, s, pl.ds(0, 3 * ch if p == 3 else ffh)]
        return rcopy(ref, ref, xs.at[p, k, dx], xr.at[p, s], z * X + lax.rem(x + dx, X), tp_i)

    def xwait(p, s):
        ref = LW.at[p, s, pl.ds(0, 3 * ch if p == 3 else ffh)]
        rcopy(ref, ref, xs.at[p, 0, 1 % X], xr.at[p, s], z * X + x, tp_i).wait_recv()

    inner = jnp.logical_and(z > 0, z < Z - 1)
    by_end = jnp.logical_or(z == 1, z == Z - 2)

    def relay(p):
        ref = LW.at[p, fs_mate, pl.ds(0, 3 * ch if p == 3 else ffh)]
        return rcopy(ref, ref, zs.at[p, 0], zr.at[p, Z - 1], xor_z(Z - 2) * X + x, tp_i)

    MIDDLE = tuple(range(2, Z - 1))

    def near(p):
        zsend(p, 1).start()

    def near_two(p):
        @pl.when(jnp.logical_not(inner))
        def _():
            for k in range(2, Z - 1):
                zsend(p, k).start()

    def far(p, ks):
        @pl.when(inner)
        def _():
            for k in ks:
                zsend(p, k).start()

    hooks = {
        0: lambda: near(1),
        1: lambda: near_two(1),
        Z - 1: lambda: near(2),
        Z: lambda: near_two(2),
    }

    def own(p):
        if p < 7:
            if p != 3:
                local_weight(p).wait()
            for dx in range(1, X):
                xsend(p, 0, dx).start()

    done = [0]

    def advance(p, k):
        last = min(p, 6) * (Z - 1) + (k if p < 7 else Z - 1)
        while done[0] < last:
            m = done[0]
            q, d = m // (Z - 1), m % (Z - 1) + 1
            zsend(q, d).wait_recv()
            if d == 1:
                @pl.when(by_end)
                def _():
                    relay(q).start()
                if q < 2:
                    far(q + 1, MIDDLE)
                if 1 <= q < 6:
                    far(q + 1, (Z - 1,))
            if m in hooks:
                hooks[m]()
            for dx in range(1, X):
                xsend(q, d, dx).start()
            if m % (Z - 1) == Z - 2 and q >= 2:
                own(q + 1)
            done[0] = m + 1

    def ag_piece(q, t):
        return XF.at[q, pl.ds(t * nb, nb)]

    def agz():
        r = ag_piece(zp, tp_i)
        return rcopy(r, r, ags.at[0], agr.at[0], fs_mate, tp_i)

    def agy(q, qi, dy):
        r = ag_piece(q, tp_i)
        return rcopy(r, r, ags.at[1 + qi * Y + dy], agr.at[1 + qi * Y + dy], fs_i, yo(dy) * 2 + core)

    def agy_wait(q, qi, dy):
        agy(q, qi, dy).wait_recv()

    def agc(q, qi, dy):
        r = ag_piece(q, lax.rem(y + Y - dy, Y) * 2 + core)
        n = 1 + 2 * Y + qi * Y + dy
        return rcopy(r, r, ags.at[n], agr.at[n], fs_i, tp_core)

    mark("tok")
    for b in range(nb):
        local_tok(b).wait()
    agz().start()
    for dy in range(1, Y):
        agy(zp, 0, dy).start()
    agc(zp, 0, 0).start()
    near(0)
    near_two(0)
    for p in range(2):
        far(p, (Z - 1,))
    for p in range(3):
        own(p)
    for n in range(2):
        local_conv(n).wait()
        LW[3, fs_i, n * ch:(n + 1) * ch] = HID[n, 0:kb, 0:ch].T
    local_weight(3).wait()
    if g.lw > ffh:
        def zero(i, c):
            for p in (0, 1, 2, 4, 5, 6):
                LW[p, i, ffh:] = jnp.zeros((g.lw - ffh, kb), BF16)
            return c
        lax.fori_loop(0, FS, zero, 0)
    GB[0:PAD] = jnp.zeros((PAD, ch), F32)
    GB[PAD + rows:] = jnp.zeros((PAD, ch), F32)
    mark("agz")
    agz().wait_recv()
    for dy in range(1, Y):
        agy(oq, 1, dy).start()
    agc(oq, 1, 0).start()
    far(0, MIDDLE)
    mark("agy0")
    for dy in range(1, Y):
        agy_wait(zp, 0, dy)
        agc(zp, 0, dy).start()
    mark("adv01")
    advance(0, 1)
    mark("agy1")
    for dy in range(1, Y):
        agy_wait(oq, 1, dy)
        agc(oq, 1, dy).start()
    mark("adv03")
    advance(0, 2)
    mark("agc")
    for dy in range(Y):
        agc(zp, 0, dy).wait_recv()
        agc(oq, 1, dy).wait_recv()
    agz().wait_send()
    for dy in range(Y):
        agc(zp, 0, dy).wait_send()
        agc(oq, 1, dy).wait_send()
        if dy:
            agy(zp, 0, dy).wait_send()
            agy(oq, 1, dy).wait_send()

    my_cell = pl.multiple_of(core * TH + y * R, 16)

    def cell_of(yy):
        return pl.multiple_of(core * TH + yy * R, 16)

    mine = pl.ds(pl.multiple_of(core * TH, 16), TH)

    def keep(s, c):
        XR[s] = XF[zp, s, mine]
        return c

    lax.fori_loop(0, FS, keep, 0)

    NR = 64

    def normalize(q, layer, put=None):
        def chunk(c, carry):
            at = pl.ds(pl.multiple_of(c * NR, NR), NR)
            total = jnp.zeros((NR, kb), F32)
            for s in range(FS):
                v = XF[q, s, at].astype(F32)
                total = total + v * v
            scale = lax.rsqrt(jnp.sum(total, axis=1, keepdims=True) / g.dim + 1e-06)
            for s in range(FS):
                v = (XF[q, s, at].astype(F32) * scale * gains[layer][s]).astype(BF16)
                if put is None:
                    XF[q, s, at] = v
                else:
                    put(s, at, v)
            return carry
        lax.fori_loop(0, rows // NR, chunk, 0)

    MR = rows // 2

    def arrived(p):
        def one(i):
            @pl.when(lax.rem(i, X) > 0)
            def _():
                xwait(p, s_of(i))
        loop(FS, one)

    def features(p, block, width):
        total = None
        for s in range(FS):
            d = lax.dot_general(block(s), LW[p, s, 0:width], NT, preferred_element_type=F32)
            total = d if total is None else total + d
        return total

    def chunks(qs, f):
        def one(t):
            q = t // (rows // MR) if qs is None else qs
            f(q, pl.ds(pl.multiple_of(lax.rem(t, rows // MR) * MR, MR), MR))
        loop((2 if qs is None else 1) * (rows // MR), one)

    def loop(n, f):
        def step(i, c):
            f(i)
            return c
        lax.fori_loop(0, n, step, 0)

    def a_copy(s, nq):
        at = pl.ds(pl.multiple_of((1 - core) * TH, 16), TH)
        here = pl.ds(0, TH)
        return rcopy(PP.at[s, pl.ds(0, nq), at], RA.at[s, pl.ds(0, nq), here], as_.at[s], ar.at[s], fs_i, tp_core)

    def b_copy(s, dy):
        return rcopy(PP.at[s, :, pl.ds(cell_of(yo(dy)), R)], RB.at[dy - 1, s],
                     bs.at[s, dy], br.at[s, dy], fs_i, yo(dy) * 2 + core)

    def c_copy(s):
        return rcopy(PP.at[s, oq, pl.ds(my_cell, R)], RC.at[s], cs_s.at[s], cr.at[s], fs_mate, tp_i)

    def d_copy(s, dy):
        return rcopy(PP.at[s, 0, mine], RD.at[dy - 1, s], ds.at[s, dy], dr.at[s, dy], fs_i, yo(dy) * 2 + core)

    def stage_a(s, nq):
        a_copy(s, nq).wait_recv()
        for q in range(nq):
            PP[s, q, mine] = (PP[s, q, mine].astype(F32) + RA[s, q].astype(F32)).astype(BF16)

    def e_copy(s):
        return rcopy(PP.at[s, oq, mine], RE.at[s], es.at[s], er.at[s], fs_mate, tp_i)

    def f_copy(s, dy):
        return rcopy(PP.at[s, zp, pl.ds(cell_of(yo(dy)), R)], RF.at[dy - 1, s],
                     fss.at[s, dy], fr.at[s, dy], fs_i, yo(dy) * 2 + core)

    turns = [False]

    def by_parity(i, first, second):
        if not turns[0]:
            first()
            return
        if isinstance(i, int):
            (second if i % 2 else first)()
        else:
            pl.when(lax.rem(i, 2) == 0)(first)
            pl.when(lax.rem(i, 2) == 1)(second)

    def stage_one(i):
        s = s_of(i)
        stage_a(s, 2)

        def even():
            for dy in range(1, Y):
                b_copy(s, dy).start()

        def odd():
            e_copy(s).start()
        by_parity(i, even, odd)

    def b_sum(s, q):
        total = PP[s, q, pl.ds(my_cell, R)].astype(F32)
        for dy in range(1, Y):
            total = total + RB[dy - 1, s, q].astype(F32)
        return total

    def stage_two(i):
        s = s_of(i)

        def even():
            for dy in range(1, Y):
                b_copy(s, dy).wait_recv()
            PP[s, oq, pl.ds(my_cell, R)] = b_sum(s, oq).astype(BF16)
            c_copy(s).start()

        def odd():
            e_copy(s).wait_recv()
            PP[s, zp, mine] = (PP[s, zp, mine].astype(F32) + RE[s].astype(F32)).astype(BF16)
            for dy in range(1, Y):
                f_copy(s, dy).start()
        by_parity(i, even, odd)

    def residual(s, total):
        return (XR[s, pl.ds(pl.multiple_of(y * R, 16), R)].astype(F32) + 0.5 * total).astype(BF16)

    def stage_three(i, put):
        s = s_of(i)

        def even():
            c_copy(s).wait_recv()
            put(s, residual(s, b_sum(s, zp) + RC[s].astype(F32)))

        def odd():
            total = PP[s, zp, pl.ds(my_cell, R)].astype(F32)
            for dy in range(1, Y):
                f_copy(s, dy).wait_recv()
                total = total + RF[dy - 1, s].astype(F32)
            put(s, residual(s, total))
        by_parity(i, even, odd)
        return s

    def sends_done(i):
        s = s_of(i)
        a_copy(s, 2).wait_send()

        def even():
            c_copy(s).wait_send()
            for dy in range(1, Y):
                b_copy(s, dy).wait_send()

        def odd():
            e_copy(s).wait_send()
            for dy in range(1, Y):
                f_copy(s, dy).wait_send()
        by_parity(i, even, odd)

    def gy_copy(q, qi, s, dy):
        r = XF.at[q, s, pl.ds(my_cell, R)]
        return rcopy(r, r, gys.at[s, dy], gyr.at[s, dy], fs_i, yo(dy) * 2 + core)

    def gc_copy(q, qi, s, dy, at):
        r = XF.at[q, s, at]
        return rcopy(r, r, gcs.at[qi, s, dy], gcr.at[qi, s, dy], fs_i, tp_core)

    def cell_from(dy):
        return pl.ds(cell_of(lax.rem(y - dy + Y, Y)), R)

    def plane_copy(s, at):
        r = XF.at[zp, s, at]
        return rcopy(r, r, gzs.at[s], gzr.at[s], fs_mate, tp_i)

    LAG_TWO, LAG_THREE = 3, 5

    def gate_rows(p0, block):
        def f(q, at):
            ACC[q, at] = features(p0, lambda s: block(q, s, at), g.ffp)
        return f

    def up_rows(p0, block):
        def f(q, at):
            v = ACC[q, at]
            HID[q, at] = (v * jax.nn.sigmoid(v) * features(p0 + 1, lambda s: block(q, s, at), g.ffp)).astype(BF16)
        return f

    def down_and_sum(p0, before_down, plan, finish, before_last, after):
        before_down()
        for j in range(Z):
            mark(f"adv_p{p0 + 2}_{j}")
            plan[j]()

            def each(e):
                i = j * X + e
                s = s_of(i)

                @pl.when(e > 0)
                def _():
                    xwait(p0 + 2, s)

                def seq(q):
                    PP[s, q] = jnp.dot(HID[q], LW[p0 + 2, s, pl.ds(0, g.ffp)], preferred_element_type=F32).astype(BF16)
                loop(2, seq)
                a_copy(s, 2).start()

                @pl.when(i >= 1)
                def _():
                    stage_one(i - 1)

                @pl.when(i >= LAG_TWO)
                def _():
                    stage_two(i - LAG_TWO)

                @pl.when(i >= LAG_THREE)
                def _():
                    finish(i - LAG_THREE)
            mark(f"down_p{p0 + 2}_{j}")
            loop(X, each)
        mark("drain_a")
        stage_one(FS - 1)
        mark("drain_b")
        for i in range(FS - LAG_TWO, FS):
            if i == FS - 1:
                mark("fill")
                before_last()
                mark("drain_b2")
            stage_two(i)
            if i >= LAG_THREE - LAG_TWO:
                finish(i + LAG_TWO - LAG_THREE)
        after()
        mark("drain_c")
        for i in range(FS + LAG_TWO - LAG_THREE, FS):
            finish(i)

    mark("norm0")
    normalize(0, 0)
    normalize(1, 0)

    def put_one(s, v):
        XF[zp, s, pl.ds(my_cell, R)] = v

    def finish_one(i):
        s = stage_three(i, put_one)
        for dy in range(1, Y):
            gy_copy(zp, 0, s, dy).start()
        gc_copy(zp, 0, s, 0, pl.ds(my_cell, R)).start()

    def from_xf(q, s, at):
        return XF[q, s, at]

    mark("adv_p0")
    advance(1, 1)
    mark("wait_p0")
    arrived(0)
    mark("adv2_p0")
    advance(1, 2)
    mark("gate_p0")
    chunks(None, gate_rows(0, from_xf))
    mark("adv_p1")
    advance(2, 1)
    mark("wait_p1")
    arrived(1)
    mark("up_p1")
    chunks(None, up_rows(0, from_xf))
    down_and_sum(
        0,
        lambda: (near(3), far(3, MIDDLE)),
        [lambda: advance(2, 1), lambda: advance(2, 2), lambda: (near_two(3), advance(2, Z - 1)), lambda: advance(3, 1)],
        finish_one,
        lambda: advance(3, Z - 1),
        lambda: (near(4), near_two(4), far(4, MIDDLE), near(5), far(5, MIDDLE)),
    )

    mark("own_arr")

    def from_y(s):
        for dy in range(1, Y):
            gy_copy(zp, 0, s, dy).wait_recv()
            gc_copy(zp, 0, s, dy, cell_from(dy)).start()
        XR[s] = XF[zp, s, mine]
    loop(FS, from_y)
    mark("own_core")
    near_two(5)
    loop(FS, sends_done)

    def one_sends(s):
        for dy in range(Y):
            if dy:
                gy_copy(zp, 0, s, dy).wait_send()
            gc_copy(zp, 0, s, dy, pl.ds(my_cell, R)).wait()
    loop(FS, one_sends)

    mark("norm1")
    normalize(zp, 1)
    mark("mix")

    arrived(3)

    def mix(q, at):
        both = features(3, lambda s: XF[zp, s, at], 2 * ch)
        GB[pl.ds(pl.multiple_of(at.start + PAD, 16), MR)] = both[:, :ch] * jax.nn.sigmoid(both[:, ch:])
    chunks(zp, mix)

    off = PAD - g.kw // 2
    lanes = 128

    def taps(t):
        at = pl.multiple_of(t * NR, NR)
        sum_one = jnp.zeros((NR, 1), F32)
        sum_two = jnp.zeros((NR, 1), F32)
        for c in range(ch // lanes):
            cols = slice(c * lanes, (c + 1) * lanes)
            window = GB[pl.ds(at, NR + 2 * PAD), cols]
            total = jnp.zeros((NR, lanes), F32)
            for r in range(8):
                taps_here = [k for k in range(g.kw) if (k + off) % 8 == r]
                shifted = window[r:max(taps_here) + off + NR]
                for k in taps_here:
                    total = total + ck[k:k + 1, cols] * shifted[k + off - r:k + off - r + NR]
            CV[pl.ds(at, NR), cols] = total
            sum_one = sum_one + jnp.sum(total, axis=1, keepdims=True)
            sum_two = sum_two + jnp.sum(total * total, axis=1, keepdims=True)
        which = lax.broadcasted_iota(jnp.int32, (NR, 128), 1)
        AB[pl.ds(at, NR)] = jnp.where(which == 0, sum_one, jnp.where(which == 1, sum_two, 0.0))
    mark("taps")
    loop(rows // NR, taps)
    mark("stats")

    def flip(t):
        at = pl.ds(pl.multiple_of(t * 128, 128), 128)
        SB[:, at] = AB[at].T[0:8]
    loop(rows // 128, flip)

    def st_copy(dt):
        return rcopy(SB, SR.at[dt - 1], sts.at[dt], st_r.at[dt], fs_i, lax.rem(tp_i + dt, TP))

    for dt in range(1, TP):
        st_copy(dt).start()
    advance(4, 1)
    for dt in range(1, TP):
        st_copy(dt).wait()

    def unflip(t):
        at = pl.ds(pl.multiple_of(t * 128, 128), 128)
        total = SB[:, at]
        for dt in range(1, TP):
            total = total + SR[dt - 1, :, at]
        AB[at] = jnp.concatenate([total, jnp.zeros((120, 128), F32)], axis=0).T
    loop(rows // 128, unflip)

    def activate(t):
        at = pl.ds(pl.multiple_of(t * NR, NR), NR)
        stats = AB[at]
        mean = stats[:, 0:1] / (ch * TP)
        var = stats[:, 1:2] / (ch * TP) - mean * mean
        v = (CV[at] - mean) * lax.rsqrt(var + 1e-05) * cg[...]
        HID[0, at, 0:ch] = (v * jax.nn.sigmoid(v)).astype(BF16)
    mark("active")
    loop(rows // NR, activate)

    def y_total(s):
        for dy in range(1, Y):
            d_copy(s, dy).wait_recv()
        own_part = PP[s, 0, mine].astype(F32)
        if Y == 2:
            return own_part + RD[0, s].astype(F32)
        total = jnp.zeros((TH, kb), F32)
        for yy in range(Y):
            slot = lax.rem(y - yy + Y, Y)
            term = RD[lax.max(slot - 1, 0), s].astype(F32)
            total = total + jnp.where(slot == 0, own_part, term)
        return total

    def mixed(i):
        s = s_of(i)
        v = (XR[s].astype(F32) + y_total(s)).astype(BF16)
        XR[s] = v
        XF[zp, s, mine] = v
        plane_copy(s, plane_rows(i)).start()
        gc_copy(zp, 0, s, 0, mine).start()

    def whole(i):
        return False

    def plane_rows(i):
        return mine if whole(i) else pl.ds(my_cell, R)

    def pass_on(i):
        s = s_of(i)
        plane_copy(s, plane_rows(i)).wait_recv()
        gc_copy(oq, 1, s, 0, plane_rows(i)).start()
        if not whole(i):
            for dy in range(1, Y):
                gy_copy(oq, 1, s, dy).start()

    def last_hop(i):
        if not whole(i):
            s = s_of(i)
            for dy in range(1, Y):
                gy_copy(oq, 1, s, dy).wait_recv()
                gc_copy(oq, 1, s, dy, cell_from(dy)).start()

    def to_y(s):
        stage_a(s, 1)
        for dy in range(1, Y):
            d_copy(s, dy).start()

    def project(i):
        s = s_of(i)
        PP[s, 0] = jnp.dot(HID[0, :, 0:ch], LW[3, s, 2 * ch:3 * ch], preferred_element_type=F32).astype(BF16)
        a_copy(s, 1).start()

        @pl.when(i >= 2)
        def _():
            to_y(s_of(i - 2))
    loop(FS, project)
    to_y(s_of(FS - 2))
    to_y(s_of(FS - 1))
    advance(4, 2)
    LAG_ON = 5
    for i in range(FS):
        mark(f"mixed_{i}")
        mixed(i)
        if i == FS - 3:
            near(6)
            far(6, MIDDLE)
        if i == FS - 1:
            near_two(6)
        if i >= LAG_ON:
            pass_on(i - LAG_ON)
        if i % 2 == 1 and i < 2 * Z:
            mark(f"mixadv_{i}")
            advance(4 + (i // 2 + 2) // (Z - 1), (i // 2 + 2) % (Z - 1) + 1)
    mark("own2")

    def own_ready(s):
        gc_copy(zp, 0, s, 0, mine).wait_recv()
    loop(FS, own_ready)

    def put_own(s, at, v):
        PP[s, 1, at] = v

    def from_own(q, s, at):
        return PP[s, 1, at]

    mark("norm2")
    normalize(zp, 2, put_own)
    left = list(range(FS - LAG_ON, FS))
    third = -(-len(left) // 3)
    mark("pass_a")
    for i in left[:third]:
        pass_on(i)
    mark("wait_p4")
    arrived(4)
    mark("gate_p4")
    chunks(zp, gate_rows(4, from_own))
    mark("pass_b")
    for i in left[third:2 * third]:
        pass_on(i)
    mark("wait_p5")
    arrived(5)
    mark("up_p5")
    chunks(zp, up_rows(4, from_own))
    mark("pass_c")
    for i in left[2 * third:]:
        pass_on(i)
    mark("adv61")
    advance(6, 1)
    mark("mixsends")

    for i in range(FS):
        last_hop(i)
    for i in range(FS):
        s = s_of(i)
        a_copy(s, 1).wait_send()
        plane_copy(s, plane_rows(i)).wait_send()
        gc_copy(zp, 0, s, 0, mine).wait_send()
        gc_copy(oq, 1, s, 0, plane_rows(i)).wait()
        for dy in range(1, Y):
            d_copy(s, dy).wait_send()
            if not whole(i):
                gy_copy(oq, 1, s, dy).wait_send()
                gc_copy(oq, 1, s, dy, cell_from(dy)).wait()
    mark("norm2b")
    normalize(oq, 2)
    mark("gate_p4b")
    chunks(oq, gate_rows(4, from_xf))
    mark("adv62")
    advance(6, 2)
    mark("up_p5b")
    chunks(oq, up_rows(4, from_xf))

    def o_copy(s, slot):
        owner = s // nb
        b = lax.rem(s, nb)
        return rcopy(XR.at[s, 0:R], out.at[pl.ds(my_cell, R), pl.ds(pl.multiple_of(b * kb, kb), kb)], os_.at[s], orr.at[b, slot], fs_i, owner)

    def put_two(s, v):
        XR[s, 0:R] = v

    def finish_two(i):
        s = stage_three(i, put_two)
        owner = s // nb

        @pl.when(owner == tp_i)
        def _():
            out[pl.ds(my_cell, R), pl.ds(pl.multiple_of(lax.rem(s, nb) * kb, kb), kb)] = XR[s, 0:R]

        @pl.when(owner != tp_i)
        def _():
            o_copy(s, lax.rem(tp_i - owner + TP, TP)).start()

    turns[0] = True
    down_and_sum(4, lambda: None, [partial(advance, 6, Z - 1)] * Z, finish_two, lambda: None, lambda: None)

    mark("out_wait")
    for b in range(nb):
        for slot in range(1, TP):
            rcopy(XR.at[0, 0:R], out.at[pl.ds(0, R), pl.ds(b * kb, kb)], os_.at[0], orr.at[b, slot], fs_i, tp_i).wait_recv()

    mark("end_sends")

    def out_sent(s):
        @pl.when(s // nb != tp_i)
        def _():
            o_copy(s, 0).wait_send()
    loop(FS, out_sent)

    loop(FS, sends_done)
    for p in range(7):
        for k in range(1, Z - 1):
            zsend(p, k).wait_send()

        @pl.when(inner)
        def _():
            zsend(p, Z - 1).wait_send()

        @pl.when(by_end)
        def _():
            relay(p).wait_send()
        for k in range(Z):
            for dx in range(1, X):
                xsend(p, k, dx).wait_send()
    mark(None)


def per_device(fs, tp, tokens, g0, wg0, wu0, wd0, g1, cv, cgate, ck, cln, co, g2, wg1, wu1, wd1):
    ws = [wg0.T, wu0.T, wd0, wg1.T, wu1.T, wd1]
    g = Plan(fs, tp, tokens.shape, wd0.shape, co.shape, ck.shape[0])
    gains = [v.reshape(fs, 1, g.kb) for v in (g0, g1, g2)]
    Z, X, Y, TP, FS = g.z, g.x, g.y, g.tp, g.fs
    dma = pltpu.SemaphoreType.DMA
    vm = pltpu.VMEM
    scratch = [
        vm((7, FS, g.lw, g.kb), BF16),
        vm((2, FS, g.rows, g.kb), BF16),
        vm((FS, g.half_rows, g.kb), BF16),
        vm((2, g.rows, g.ffp), F32),
        vm((2, g.rows, g.ffp), BF16),
        vm((FS, 2, g.rows, g.kb), BF16),
        vm((FS, 2, g.half_rows, g.kb), BF16),
        vm((Y - 1, FS, 2, g.cell, g.kb), BF16),
        vm((FS, g.cell, g.kb), BF16),
        vm((Y - 1, FS, g.half_rows, g.kb), BF16),
        vm((FS, g.half_rows, g.kb), BF16),
        vm((Y - 1, FS, g.cell, g.kb), BF16),
        vm((g.rows + 2 * PAD, g.ch), F32),
        vm((g.rows, g.ch), F32),
        vm((8, g.rows), F32),
        vm((TP - 1, 8, g.rows), F32),
        vm((g.rows, 128), F32),
        dma((7,)), dma((2,)), dma((g.nb,)),
        dma((7, Z)), dma((7, Z)),
        dma((7, Z, X)), dma((7, FS)),
        dma((1 + 4 * Y,)), dma((1 + 4 * Y,)),
        dma((FS,)), dma((FS,)),
        dma((FS, Y)), dma((FS, Y)),
        dma((FS,)), dma((FS,)),
        dma((FS, Y)), dma((FS, Y)),
        dma((FS,)), dma((FS,)),
        dma((FS, Y)), dma((FS, Y)),
        dma((FS, Y)), dma((FS, Y)),
        dma((FS,)), dma((FS,)),
        dma((2, FS, Y)), dma((2, FS, Y)),
        dma((TP,)), dma((TP,)),
        dma((FS,)), dma((g.nb, TP)),
    ]
    anyspace = pl.BlockSpec(memory_space=pl.ANY)
    vmem = pl.BlockSpec(memory_space=pltpu.VMEM)
    res = pl.pallas_call(
        partial(body, g),
        out_shape=jax.ShapeDtypeStruct((g.rows, g.nb * g.kb), BF16),
        in_specs=[anyspace] * 10 + [vmem] * 5,
        out_specs=vmem,
        scratch_shapes=scratch,
        compiler_params=pltpu.CompilerParams(
            collective_id=0, has_side_effects=True, vmem_limit_bytes=67043328
        ),
        name="layer",
    )(tokens, *ws, cv, cgate, co, *gains, ck, cln.reshape(1, -1))
    return res


def solution(mesh):
    fs, tp = mesh.shape["fs"], mesh.shape["tp"]
    both = P("fs", "tp")
    down = P("tp", "fs")
    in_specs = (both, P(), both, both, down, P(), both, both, P(None, "tp"), P("tp"), down, P(), both, both, down)
    return jax.shard_map(
        partial(per_device, fs, tp), mesh=mesh, in_specs=in_specs, out_specs=both, check_vma=False
    )
```

```python
from functools import partial

import jax
import jax.numpy as jnp
from jax import lax
from jax.experimental import pallas as pl
from jax.experimental.pallas import tpu as pltpu
from jax.sharding import PartitionSpec as P

F32 = jnp.float32
BF16 = jnp.bfloat16
MESH = pl.DeviceIdType.MESH
NT = (((1,), (1,)), ((), ()))
PAD = 16


def split_fs(total):
    inner = 1
    while total % (inner * 2) == 0 and (inner * 2) ** 2 <= total:
        inner *= 2
    return total // inner, inner


class Plan:
    def __init__(self, fs, tp, tok, ws, co, kernel_rows):
        self.fs, self.tp = fs, tp
        self.z, self.x = split_fs(fs)
        self.y = tp // 2
        self.rows, width = tok
        self.kb = ws[1]
        self.nb = width // self.kb
        self.ffh = ws[0] // 2
        self.ch = co[0]
        unit = 256 if self.ch % 256 == 0 else 128
        self.ffp = -(-self.ffh // unit) * unit
        self.lw = max(self.ffp, 3 * self.ch)
        self.half_rows = self.rows // 2
        self.cell = self.half_rows // self.y
        self.kw = kernel_rows
        self.turn = ws[0] % 128 == 0
        self.dim = self.kb * fs


class Marks:
    def __init__(self):
        self.open = None

    def __call__(self, name):
        if self.open is not None:
            self.open.__exit__(None, None, None)
        self.open = None
        if name is not None:
            self.open = jax.named_scope(name)
            self.open.__enter__()


def body(g, *refs):
    mark = Marks()
    mark("entry")
    (tok, *ws, cv, cgate, co, ga, gb, gc, ck, cg, out) = refs[:16]
    (LW, XF, XR, ACC, HID, PP, RA, RB, RC, RD, RE, RF, GB, CV, SB, SR, AB, ST, TW) = refs[16:35]
    gains = (ga, gb, gc)
    (s_loc, s_conv, s_turn, s_tok, zs, zr, xs, xr, ags, agr, as_, ar, bs, br, cs_s, cr, ds, dr, es, er, fss, fr, gys, gyr, gzs, gzr, gcs, gcr, sts, st_r, os_, orr) = refs[35:]
    Z, X, Y, TP, FS = g.z, g.x, g.y, g.tp, g.fs
    rows, kb, nb, ffh, ch = g.rows, g.kb, g.nb, g.ffh, g.ch
    TH, R = g.half_rows, g.cell
    fs_i, tp_i = lax.axis_index("fs"), lax.axis_index("tp")
    z, x = fs_i // X, fs_i % X
    y, core = tp_i // 2, tp_i % 2
    zp = z % 2
    oq = 1 - zp
    zb = z - zp
    zmate = zb + oq
    fs_mate = zmate * X + x
    tp_core = y * 2 + 1 - core

    def zx(j):
        if isinstance(j, int):
            hi, lo = j - j % 2, j % 2
        else:
            hi, lo = j - lax.rem(j, 2), lax.rem(j, 2)
        return xor2(zb, hi) + lo

    def xor2(a, b):
        r, bit = 0, 2
        while bit < Z:
            abit = lax.rem(a // bit, 2)
            bbit = (b // bit) % 2 if isinstance(b, int) else lax.rem(b // bit, 2)
            r = r + bit * lax.rem(abit + bbit, 2)
            bit *= 2
        return r

    def xor_z(k):
        r, bit = 0, 1
        while bit < Z:
            r = r + bit * lax.rem(lax.rem(z // bit, 2) + (k // bit) % 2, 2)
            bit *= 2
        return r

    def s_of(i):
        if isinstance(i, int):
            return zx(i // X) * X + lax.rem(x + i % X, X)
        return zx(i // X) * X + lax.rem(x + lax.rem(i, X), X)

    def rcopy(src, dst, ssem, rsem, fs_to, tp_to):
        return pltpu.make_async_remote_copy(
            src_ref=src, dst_ref=dst, send_sem=ssem, recv_sem=rsem,
            device_id=(fs_to, tp_to), device_id_type=MESH,
        )

    def yo(dy):
        return lax.rem(y + dy, Y)

    bar = pltpu.get_barrier_semaphore()
    peers = [(xor_z(k) * X + x, tp_i) for k in range(1, Z)]
    peers += [(z * X + lax.rem(x + dx, X), tp_i) for dx in range(1, X)]
    peers += [(fs_i, lax.rem(tp_i + dt, TP)) for dt in range(1, TP)]
    for f_to, t_to in peers:
        pl.semaphore_signal(bar, inc=1, device_id=(f_to, t_to), device_id_type=MESH)

    turned = (4, 5) if g.turn else ()

    def half_of(p, parity):
        at = pl.ds(pl.multiple_of(parity * ffh, 16), ffh)
        if p in turned:
            return TW.at[p - 4, at]
        return ws[p if p < 3 else p - 1].at[at]

    def stage_turn(n):
        return pltpu.make_async_copy(ws[3 + n], ST.at[n], s_turn.at[n])

    def local_weight(p):
        if p == 3:
            return pltpu.make_async_copy(co, LW.at[3, fs_i, pl.ds(2 * ch, ch)], s_loc.at[p])
        src = half_of(p, zp)
        return pltpu.make_async_copy(src, LW.at[p, fs_i, pl.ds(0, ffh)], s_loc.at[p])

    def local_tok(b):
        return pltpu.make_async_copy(
            tok.at[:, pl.ds(b * kb, kb)], XF.at[zp, tp_i * nb + b], s_tok.at[b]
        )

    for b in range(nb):
        local_tok(b).start()
    for p in range(7):
        if p in turned:
            stage_turn(p - 4).start()
        else:
            local_weight(p).start()

    def local_conv(n):
        return pltpu.make_async_copy((cv, cgate)[n], HID.at[n, pl.ds(0, kb), pl.ds(0, ch)], s_conv.at[n])

    for n in range(2):
        local_conv(n).start()
    pl.semaphore_wait(bar, len(peers))

    def zsend(p, k):
        to = xor_z(k)
        if p == 3:
            src = dst = LW.at[3, fs_i, pl.ds(0, 3 * ch)]
        else:
            src = half_of(p, lax.rem(to, 2))
            dst = LW.at[p, fs_i, pl.ds(0, ffh)]
        return rcopy(src, dst, zs.at[p, k], zr.at[p, k], to * X + x, tp_i)

    def xsend(p, k, dx):
        s = (xor_z(k) if k else z) * X + x
        ref = LW.at[p, s, pl.ds(0, 3 * ch if p == 3 else ffh)]
        return rcopy(ref, ref, xs.at[p, k, dx], xr.at[p, s], z * X + lax.rem(x + dx, X), tp_i)

    def xwait(p, s):
        ref = LW.at[p, s, pl.ds(0, 3 * ch if p == 3 else ffh)]
        rcopy(ref, ref, xs.at[p, 0, 1 % X], xr.at[p, s], z * X + x, tp_i).wait_recv()

    inner = jnp.logical_and(z > 0, z < Z - 1)
    by_end = jnp.logical_or(z == 1, z == Z - 2)

    def relay(p):
        ref = LW.at[p, fs_mate, pl.ds(0, 3 * ch if p == 3 else ffh)]
        return rcopy(ref, ref, zs.at[p, 0], zr.at[p, Z - 1], xor_z(Z - 2) * X + x, tp_i)

    MIDDLE = tuple(range(2, Z - 1))

    def near(p):
        zsend(p, 1).start()

    def near_two(p):
        @pl.when(jnp.logical_not(inner))
        def _():
            for k in range(2, Z - 1):
                zsend(p, k).start()

    def far(p, ks):
        @pl.when(inner)
        def _():
            for k in ks:
                zsend(p, k).start()

    hooks = {
        0: lambda: near(1),
        1: lambda: near_two(1),
        Z - 1: lambda: near(2),
        Z: lambda: near_two(2),
    }

    def own(p):
        if p < 7:
            if p != 3 and p not in turned:
                local_weight(p).wait()
            for dx in range(1, X):
                xsend(p, 0, dx).start()

    done = [0]

    def advance(p, k):
        last = min(p, 6) * (Z - 1) + (k if p < 7 else Z - 1)
        while done[0] < last:
            m = done[0]
            q, d = m // (Z - 1), m % (Z - 1) + 1
            zsend(q, d).wait_recv()
            if d == 1:
                @pl.when(by_end)
                def _():
                    relay(q).start()
                if q < 2:
                    far(q + 1, MIDDLE)
                if 1 <= q < 6:
                    far(q + 1, (Z - 1,))
            if m in hooks:
                hooks[m]()
            for dx in range(1, X):
                xsend(q, d, dx).start()
            if m % (Z - 1) == Z - 2 and q >= 2:
                own(q + 1)
            done[0] = m + 1

    def ag_piece(q, t):
        return XF.at[q, pl.ds(t * nb, nb)]

    def agz():
        r = ag_piece(zp, tp_i)
        return rcopy(r, r, ags.at[0], agr.at[0], fs_mate, tp_i)

    def agy(q, qi, dy):
        r = ag_piece(q, tp_i)
        return rcopy(r, r, ags.at[1 + qi * Y + dy], agr.at[1 + qi * Y + dy], fs_i, yo(dy) * 2 + core)

    def agy_wait(q, qi, dy):
        agy(q, qi, dy).wait_recv()

    def agc(q, qi, dy):
        r = ag_piece(q, lax.rem(y + Y - dy, Y) * 2 + core)
        n = 1 + 2 * Y + qi * Y + dy
        return rcopy(r, r, ags.at[n], agr.at[n], fs_i, tp_core)

    mark("tok")
    for b in range(nb):
        local_tok(b).wait()
    agz().start()
    for dy in range(1, Y):
        agy(zp, 0, dy).start()
    agc(zp, 0, 0).start()
    near(0)
    near_two(0)
    for p in range(2):
        far(p, (Z - 1,))
    for p in range(3):
        own(p)
    for n in range(2):
        local_conv(n).wait()
        LW[3, fs_i, n * ch:(n + 1) * ch] = HID[n, 0:kb, 0:ch].T
    local_weight(3).wait()
    if g.lw > ffh:
        def zero(i, c):
            for p in (0, 1, 2, 4, 5, 6):
                LW[p, i, ffh:] = jnp.zeros((g.lw - ffh, kb), BF16)
            return c
        lax.fori_loop(0, FS, zero, 0)
    for p in turned:
        n = p - 4
        stage_turn(n).wait()

        def turn(i, c):
            at = pl.ds(pl.multiple_of(i * 128, 128), 128)
            TW[n, at] = ST[n, :, at].T
            return c
        lax.fori_loop(0, 2 * ffh // 128, turn, 0)
        LW[p, fs_i, 0:ffh] = TW[n, pl.ds(pl.multiple_of(zp * ffh, 16), ffh)]
    GB[0:PAD] = jnp.zeros((PAD, ch), F32)
    GB[PAD + rows:] = jnp.zeros((PAD, ch), F32)
    mark("agz")
    agz().wait_recv()
    for dy in range(1, Y):
        agy(oq, 1, dy).start()
    agc(oq, 1, 0).start()
    far(0, MIDDLE)
    mark("agy0")
    for dy in range(1, Y):
        agy_wait(zp, 0, dy)
        agc(zp, 0, dy).start()
    mark("adv01")
    advance(0, 1)
    mark("agy1")
    for dy in range(1, Y):
        agy_wait(oq, 1, dy)
        agc(oq, 1, dy).start()
    mark("adv03")
    advance(0, 2)
    mark("agc")
    for dy in range(Y):
        agc(zp, 0, dy).wait_recv()
        agc(oq, 1, dy).wait_recv()
    agz().wait_send()
    for dy in range(Y):
        agc(zp, 0, dy).wait_send()
        agc(oq, 1, dy).wait_send()
        if dy:
            agy(zp, 0, dy).wait_send()
            agy(oq, 1, dy).wait_send()

    my_cell = pl.multiple_of(core * TH + y * R, 16)

    def cell_of(yy):
        return pl.multiple_of(core * TH + yy * R, 16)

    mine = pl.ds(pl.multiple_of(core * TH, 16), TH)

    def keep(s, c):
        XR[s] = XF[zp, s, mine]
        return c

    lax.fori_loop(0, FS, keep, 0)

    NR = 64

    def normalize(q, layer, put=None):
        def chunk(c, carry):
            at = pl.ds(pl.multiple_of(c * NR, NR), NR)
            total = jnp.zeros((NR, kb), F32)
            for s in range(FS):
                v = XF[q, s, at].astype(F32)
                total = total + v * v
            scale = lax.rsqrt(jnp.sum(total, axis=1, keepdims=True) / g.dim + 1e-06)
            for s in range(FS):
                v = (XF[q, s, at].astype(F32) * scale * gains[layer][s]).astype(BF16)
                if put is None:
                    XF[q, s, at] = v
                else:
                    put(s, at, v)
            return carry
        lax.fori_loop(0, rows // NR, chunk, 0)

    MR = rows // 2

    def arrived(p):
        def one(i):
            @pl.when(lax.rem(i, X) > 0)
            def _():
                xwait(p, s_of(i))
        loop(FS, one)

    def features(p, block, width):
        total = None
        for s in range(FS):
            d = lax.dot_general(block(s), LW[p, s, 0:width], NT, preferred_element_type=F32)
            total = d if total is None else total + d
        return total

    def chunks(qs, f):
        def one(t):
            q = t // (rows // MR) if qs is None else qs
            f(q, pl.ds(pl.multiple_of(lax.rem(t, rows // MR) * MR, MR), MR))
        loop((2 if qs is None else 1) * (rows // MR), one)

    def loop(n, f):
        def step(i, c):
            f(i)
            return c
        lax.fori_loop(0, n, step, 0)

    def a_copy(s, nq):
        at = pl.ds(pl.multiple_of((1 - core) * TH, 16), TH)
        here = pl.ds(0, TH)
        return rcopy(PP.at[s, pl.ds(0, nq), at], RA.at[s, pl.ds(0, nq), here], as_.at[s], ar.at[s], fs_i, tp_core)

    def b_copy(s, dy):
        return rcopy(PP.at[s, :, pl.ds(cell_of(yo(dy)), R)], RB.at[dy - 1, s],
                     bs.at[s, dy], br.at[s, dy], fs_i, yo(dy) * 2 + core)

    def c_copy(s):
        return rcopy(PP.at[s, oq, pl.ds(my_cell, R)], RC.at[s], cs_s.at[s], cr.at[s], fs_mate, tp_i)

    def d_copy(s, dy):
        return rcopy(PP.at[s, 0, mine], RD.at[dy - 1, s], ds.at[s, dy], dr.at[s, dy], fs_i, yo(dy) * 2 + core)

    def stage_a(s, nq):
        a_copy(s, nq).wait_recv()
        for q in range(nq):
            PP[s, q, mine] = (PP[s, q, mine].astype(F32) + RA[s, q].astype(F32)).astype(BF16)

    def e_copy(s):
        return rcopy(PP.at[s, oq, mine], RE.at[s], es.at[s], er.at[s], fs_mate, tp_i)

    def f_copy(s, dy):
        return rcopy(PP.at[s, zp, pl.ds(cell_of(yo(dy)), R)], RF.at[dy - 1, s],
                     fss.at[s, dy], fr.at[s, dy], fs_i, yo(dy) * 2 + core)

    turns = [False]

    def by_parity(i, first, second):
        if not turns[0]:
            first()
            return
        if isinstance(i, int):
            (second if i % 2 else first)()
        else:
            pl.when(lax.rem(i, 2) == 0)(first)
            pl.when(lax.rem(i, 2) == 1)(second)

    def stage_one(i):
        s = s_of(i)
        stage_a(s, 2)

        def even():
            for dy in range(1, Y):
                b_copy(s, dy).start()

        def odd():
            e_copy(s).start()
        by_parity(i, even, odd)

    def b_sum(s, q):
        total = PP[s, q, pl.ds(my_cell, R)].astype(F32)
        for dy in range(1, Y):
            total = total + RB[dy - 1, s, q].astype(F32)
        return total

    def stage_two(i):
        s = s_of(i)

        def even():
            for dy in range(1, Y):
                b_copy(s, dy).wait_recv()
            PP[s, oq, pl.ds(my_cell, R)] = b_sum(s, oq).astype(BF16)
            c_copy(s).start()

        def odd():
            e_copy(s).wait_recv()
            PP[s, zp, mine] = (PP[s, zp, mine].astype(F32) + RE[s].astype(F32)).astype(BF16)
            for dy in range(1, Y):
                f_copy(s, dy).start()
        by_parity(i, even, odd)

    def residual(s, total):
        return (XR[s, pl.ds(pl.multiple_of(y * R, 16), R)].astype(F32) + 0.5 * total).astype(BF16)

    def stage_three(i, put):
        s = s_of(i)

        def even():
            c_copy(s).wait_recv()
            put(s, residual(s, b_sum(s, zp) + RC[s].astype(F32)))

        def odd():
            total = PP[s, zp, pl.ds(my_cell, R)].astype(F32)
            for dy in range(1, Y):
                f_copy(s, dy).wait_recv()
                total = total + RF[dy - 1, s].astype(F32)
            put(s, residual(s, total))
        by_parity(i, even, odd)
        return s

    def sends_done(i):
        s = s_of(i)
        a_copy(s, 2).wait_send()

        def even():
            c_copy(s).wait_send()
            for dy in range(1, Y):
                b_copy(s, dy).wait_send()

        def odd():
            e_copy(s).wait_send()
            for dy in range(1, Y):
                f_copy(s, dy).wait_send()
        by_parity(i, even, odd)

    def gy_copy(q, qi, s, dy):
        r = XF.at[q, s, pl.ds(my_cell, R)]
        return rcopy(r, r, gys.at[s, dy], gyr.at[s, dy], fs_i, yo(dy) * 2 + core)

    def gc_copy(q, qi, s, dy, at):
        r = XF.at[q, s, at]
        return rcopy(r, r, gcs.at[qi, s, dy], gcr.at[qi, s, dy], fs_i, tp_core)

    def cell_from(dy):
        return pl.ds(cell_of(lax.rem(y - dy + Y, Y)), R)

    def plane_copy(s, at):
        r = XF.at[zp, s, at]
        return rcopy(r, r, gzs.at[s], gzr.at[s], fs_mate, tp_i)

    LAG_TWO, LAG_THREE = 3, 5

    def gate_rows(p0, block):
        def f(q, at):
            ACC[q, at] = features(p0, lambda s: block(q, s, at), g.ffp)
        return f

    def up_rows(p0, block):
        def f(q, at):
            v = ACC[q, at]
            HID[q, at] = (v * jax.nn.sigmoid(v) * features(p0 + 1, lambda s: block(q, s, at), g.ffp)).astype(BF16)
        return f

    def down_and_sum(p0, before_down, plan, finish, before_last, after):
        before_down()
        for j in range(Z):
            mark(f"adv_p{p0 + 2}_{j}")
            plan[j]()

            def each(e):
                i = j * X + e
                s = s_of(i)

                @pl.when(e > 0)
                def _():
                    xwait(p0 + 2, s)

                def seq(q):
                    PP[s, q] = jnp.dot(HID[q], LW[p0 + 2, s, pl.ds(0, g.ffp)], preferred_element_type=F32).astype(BF16)
                loop(2, seq)
                a_copy(s, 2).start()

                @pl.when(i >= 1)
                def _():
                    stage_one(i - 1)

                @pl.when(i >= LAG_TWO)
                def _():
                    stage_two(i - LAG_TWO)

                @pl.when(i >= LAG_THREE)
                def _():
                    finish(i - LAG_THREE)
            mark(f"down_p{p0 + 2}_{j}")
            loop(X, each)
        mark("drain_a")
        stage_one(FS - 1)
        mark("drain_b")
        for i in range(FS - LAG_TWO, FS):
            if i == FS - 1:
                mark("fill")
                before_last()
                mark("drain_b2")
            stage_two(i)
            if i >= LAG_THREE - LAG_TWO:
                finish(i + LAG_TWO - LAG_THREE)
        after()
        mark("drain_c")
        for i in range(FS + LAG_TWO - LAG_THREE, FS):
            finish(i)

    mark("norm0")
    normalize(0, 0)
    normalize(1, 0)

    def put_one(s, v):
        XF[zp, s, pl.ds(my_cell, R)] = v

    def finish_one(i):
        s = stage_three(i, put_one)
        for dy in range(1, Y):
            gy_copy(zp, 0, s, dy).start()
        gc_copy(zp, 0, s, 0, pl.ds(my_cell, R)).start()

    def from_xf(q, s, at):
        return XF[q, s, at]

    mark("adv_p0")
    advance(1, 1)
    mark("wait_p0")
    arrived(0)
    mark("adv2_p0")
    advance(1, 2)
    mark("gate_p0")
    chunks(None, gate_rows(0, from_xf))
    mark("adv_p1")
    advance(2, 1)
    mark("wait_p1")
    arrived(1)
    mark("up_p1")
    chunks(None, up_rows(0, from_xf))
    down_and_sum(
        0,
        lambda: (near(3), far(3, MIDDLE)),
        [lambda: advance(2, 1), lambda: advance(2, 2), lambda: (near_two(3), advance(2, Z - 1)), lambda: advance(3, 1)],
        finish_one,
        lambda: advance(3, Z - 1),
        lambda: (near(4), near_two(4), far(4, MIDDLE), near(5), far(5, MIDDLE)),
    )

    mark("own_arr")

    def from_y(s):
        for dy in range(1, Y):
            gy_copy(zp, 0, s, dy).wait_recv()
            gc_copy(zp, 0, s, dy, cell_from(dy)).start()
        XR[s] = XF[zp, s, mine]
    loop(FS, from_y)
    mark("own_core")
    near_two(5)
    loop(FS, sends_done)

    def one_sends(s):
        for dy in range(Y):
            if dy:
                gy_copy(zp, 0, s, dy).wait_send()
            gc_copy(zp, 0, s, dy, pl.ds(my_cell, R)).wait()
    loop(FS, one_sends)

    mark("norm1")
    normalize(zp, 1)
    mark("mix")

    arrived(3)

    def mix(q, at):
        both = features(3, lambda s: XF[zp, s, at], 2 * ch)
        GB[pl.ds(pl.multiple_of(at.start + PAD, 16), MR)] = both[:, :ch] * jax.nn.sigmoid(both[:, ch:])
    chunks(zp, mix)

    off = PAD - g.kw // 2
    lanes = 128

    def taps(t):
        at = pl.multiple_of(t * NR, NR)
        sum_one = jnp.zeros((NR, 1), F32)
        sum_two = jnp.zeros((NR, 1), F32)
        for c in range(ch // lanes):
            cols = slice(c * lanes, (c + 1) * lanes)
            window = GB[pl.ds(at, NR + 2 * PAD), cols]
            total = jnp.zeros((NR, lanes), F32)
            for r in range(8):
                taps_here = [k for k in range(g.kw) if (k + off) % 8 == r]
                shifted = window[r:max(taps_here) + off + NR]
                for k in taps_here:
                    total = total + ck[k:k + 1, cols] * shifted[k + off - r:k + off - r + NR]
            CV[pl.ds(at, NR), cols] = total
            sum_one = sum_one + jnp.sum(total, axis=1, keepdims=True)
            sum_two = sum_two + jnp.sum(total * total, axis=1, keepdims=True)
        which = lax.broadcasted_iota(jnp.int32, (NR, 128), 1)
        AB[pl.ds(at, NR)] = jnp.where(which == 0, sum_one, jnp.where(which == 1, sum_two, 0.0))
    mark("taps")
    loop(rows // NR, taps)
    mark("stats")

    def flip(t):
        at = pl.ds(pl.multiple_of(t * 128, 128), 128)
        SB[:, at] = AB[at].T[0:8]
    loop(rows // 128, flip)

    def st_copy(dt):
        return rcopy(SB, SR.at[dt - 1], sts.at[dt], st_r.at[dt], fs_i, lax.rem(tp_i + dt, TP))

    for dt in range(1, TP):
        st_copy(dt).start()
    advance(4, 1)
    for dt in range(1, TP):
        st_copy(dt).wait()

    def unflip(t):
        at = pl.ds(pl.multiple_of(t * 128, 128), 128)
        total = SB[:, at]
        for dt in range(1, TP):
            total = total + SR[dt - 1, :, at]
        AB[at] = jnp.concatenate([total, jnp.zeros((120, 128), F32)], axis=0).T
    loop(rows // 128, unflip)

    def activate(t):
        at = pl.ds(pl.multiple_of(t * NR, NR), NR)
        stats = AB[at]
        mean = stats[:, 0:1] / (ch * TP)
        var = stats[:, 1:2] / (ch * TP) - mean * mean
        v = (CV[at] - mean) * lax.rsqrt(var + 1e-05) * cg[...]
        HID[0, at, 0:ch] = (v * jax.nn.sigmoid(v)).astype(BF16)
    mark("active")
    loop(rows // NR, activate)

    def y_total(s):
        for dy in range(1, Y):
            d_copy(s, dy).wait_recv()
        own_part = PP[s, 0, mine].astype(F32)
        if Y == 2:
            return own_part + RD[0, s].astype(F32)
        total = jnp.zeros((TH, kb), F32)
        for yy in range(Y):
            slot = lax.rem(y - yy + Y, Y)
            term = RD[lax.max(slot - 1, 0), s].astype(F32)
            total = total + jnp.where(slot == 0, own_part, term)
        return total

    def mixed(i):
        s = s_of(i)
        v = (XR[s].astype(F32) + y_total(s)).astype(BF16)
        XR[s] = v
        XF[zp, s, mine] = v
        plane_copy(s, plane_rows(i)).start()
        gc_copy(zp, 0, s, 0, mine).start()

    def whole(i):
        return False

    def plane_rows(i):
        return mine if whole(i) else pl.ds(my_cell, R)

    def pass_on(i):
        s = s_of(i)
        plane_copy(s, plane_rows(i)).wait_recv()
        gc_copy(oq, 1, s, 0, plane_rows(i)).start()
        if not whole(i):
            for dy in range(1, Y):
                gy_copy(oq, 1, s, dy).start()

    def last_hop(i):
        if not whole(i):
            s = s_of(i)
            for dy in range(1, Y):
                gy_copy(oq, 1, s, dy).wait_recv()
                gc_copy(oq, 1, s, dy, cell_from(dy)).start()

    def to_y(s):
        stage_a(s, 1)
        for dy in range(1, Y):
            d_copy(s, dy).start()

    def project(i):
        s = s_of(i)
        PP[s, 0] = jnp.dot(HID[0, :, 0:ch], LW[3, s, 2 * ch:3 * ch], preferred_element_type=F32).astype(BF16)
        a_copy(s, 1).start()

        @pl.when(i >= 2)
        def _():
            to_y(s_of(i - 2))
    loop(FS, project)
    to_y(s_of(FS - 2))
    to_y(s_of(FS - 1))
    advance(4, 2)
    LAG_ON = 5
    for i in range(FS):
        mark(f"mixed_{i}")
        mixed(i)
        if i == FS - 3:
            near(6)
            far(6, MIDDLE)
        if i == FS - 1:
            near_two(6)
        if i >= LAG_ON:
            pass_on(i - LAG_ON)
        if i % 2 == 1 and i < 2 * Z:
            mark(f"mixadv_{i}")
            advance(4 + (i // 2 + 2) // (Z - 1), (i // 2 + 2) % (Z - 1) + 1)
    mark("own2")

    def own_ready(s):
        gc_copy(zp, 0, s, 0, mine).wait_recv()
    loop(FS, own_ready)

    def put_own(s, at, v):
        PP[s, 1, at] = v

    def from_own(q, s, at):
        return PP[s, 1, at]

    mark("norm2")
    normalize(zp, 2, put_own)
    left = list(range(FS - LAG_ON, FS))
    third = -(-len(left) // 3)
    mark("pass_a")
    for i in left[:third]:
        pass_on(i)
    mark("wait_p4")
    arrived(4)
    mark("gate_p4")
    chunks(zp, gate_rows(4, from_own))
    mark("pass_b")
    for i in left[third:2 * third]:
        pass_on(i)
    mark("wait_p5")
    arrived(5)
    mark("up_p5")
    chunks(zp, up_rows(4, from_own))
    mark("pass_c")
    for i in left[2 * third:]:
        pass_on(i)
    mark("adv61")
    advance(6, 1)
    mark("mixsends")

    for i in range(FS):
        last_hop(i)
    for i in range(FS):
        s = s_of(i)
        a_copy(s, 1).wait_send()
        plane_copy(s, plane_rows(i)).wait_send()
        gc_copy(zp, 0, s, 0, mine).wait_send()
        gc_copy(oq, 1, s, 0, plane_rows(i)).wait()
        for dy in range(1, Y):
            d_copy(s, dy).wait_send()
            if not whole(i):
                gy_copy(oq, 1, s, dy).wait_send()
                gc_copy(oq, 1, s, dy, cell_from(dy)).wait()
    mark("norm2b")
    normalize(oq, 2)
    mark("gate_p4b")
    chunks(oq, gate_rows(4, from_xf))
    mark("adv62")
    advance(6, 2)
    mark("up_p5b")
    chunks(oq, up_rows(4, from_xf))

    def o_copy(s, slot):
        owner = s // nb
        b = lax.rem(s, nb)
        return rcopy(XR.at[s, 0:R], out.at[pl.ds(my_cell, R), pl.ds(pl.multiple_of(b * kb, kb), kb)], os_.at[s], orr.at[b, slot], fs_i, owner)

    def put_two(s, v):
        XR[s, 0:R] = v

    def finish_two(i):
        s = stage_three(i, put_two)
        owner = s // nb

        @pl.when(owner == tp_i)
        def _():
            out[pl.ds(my_cell, R), pl.ds(pl.multiple_of(lax.rem(s, nb) * kb, kb), kb)] = XR[s, 0:R]

        @pl.when(owner != tp_i)
        def _():
            o_copy(s, lax.rem(tp_i - owner + TP, TP)).start()

    turns[0] = True
    down_and_sum(4, lambda: None, [partial(advance, 6, Z - 1)] * Z, finish_two, lambda: None, lambda: None)

    mark("out_wait")
    for b in range(nb):
        for slot in range(1, TP):
            rcopy(XR.at[0, 0:R], out.at[pl.ds(0, R), pl.ds(b * kb, kb)], os_.at[0], orr.at[b, slot], fs_i, tp_i).wait_recv()

    mark("end_sends")

    def out_sent(s):
        @pl.when(s // nb != tp_i)
        def _():
            o_copy(s, 0).wait_send()
    loop(FS, out_sent)

    loop(FS, sends_done)
    for p in range(7):
        for k in range(1, Z - 1):
            zsend(p, k).wait_send()

        @pl.when(inner)
        def _():
            zsend(p, Z - 1).wait_send()

        @pl.when(by_end)
        def _():
            relay(p).wait_send()
        for k in range(Z):
            for dx in range(1, X):
                xsend(p, k, dx).wait_send()
    mark(None)


def per_device(fs, tp, tokens, g0, wg0, wu0, wd0, g1, cv, cgate, ck, cln, co, g2, wg1, wu1, wd1):
    g = Plan(fs, tp, tokens.shape, wd0.shape, co.shape, ck.shape[0])
    late = [wg1, wu1] if g.turn else [wg1.T, wu1.T]
    ws = [wg0.T, wu0.T, wd0, *late, wd1]
    gains = [v.reshape(fs, 1, g.kb) for v in (g0, g1, g2)]
    Z, X, Y, TP, FS = g.z, g.x, g.y, g.tp, g.fs
    dma = pltpu.SemaphoreType.DMA
    vm = pltpu.VMEM
    scratch = [
        vm((7, FS, g.lw, g.kb), BF16),
        vm((2, FS, g.rows, g.kb), BF16),
        vm((FS, g.half_rows, g.kb), BF16),
        vm((2, g.rows, g.ffp), F32),
        vm((2, g.rows, g.ffp), BF16),
        vm((FS, 2, g.rows, g.kb), BF16),
        vm((FS, 2, g.half_rows, g.kb), BF16),
        vm((Y - 1, FS, 2, g.cell, g.kb), BF16),
        vm((FS, g.cell, g.kb), BF16),
        vm((Y - 1, FS, g.half_rows, g.kb), BF16),
        vm((FS, g.half_rows, g.kb), BF16),
        vm((Y - 1, FS, g.cell, g.kb), BF16),
        vm((g.rows + 2 * PAD, g.ch), F32),
        vm((g.rows, g.ch), F32),
        vm((8, g.rows), F32),
        vm((TP - 1, 8, g.rows), F32),
        vm((g.rows, 128), F32),
        vm((2,) + late[0].shape if g.turn else (2, 16, 128), BF16),
        vm((2,) + late[0].shape[::-1] if g.turn else (2, 16, 128), BF16),
        dma((7,)), dma((2,)), dma((2,)), dma((g.nb,)),
        dma((7, Z)), dma((7, Z)),
        dma((7, Z, X)), dma((7, FS)),
        dma((1 + 4 * Y,)), dma((1 + 4 * Y,)),
        dma((FS,)), dma((FS,)),
        dma((FS, Y)), dma((FS, Y)),
        dma((FS,)), dma((FS,)),
        dma((FS, Y)), dma((FS, Y)),
        dma((FS,)), dma((FS,)),
        dma((FS, Y)), dma((FS, Y)),
        dma((FS, Y)), dma((FS, Y)),
        dma((FS,)), dma((FS,)),
        dma((2, FS, Y)), dma((2, FS, Y)),
        dma((TP,)), dma((TP,)),
        dma((FS,)), dma((g.nb, TP)),
    ]
    anyspace = pl.BlockSpec(memory_space=pl.ANY)
    vmem = pl.BlockSpec(memory_space=pltpu.VMEM)
    res = pl.pallas_call(
        partial(body, g),
        out_shape=jax.ShapeDtypeStruct((g.rows, g.nb * g.kb), BF16),
        in_specs=[anyspace] * 10 + [vmem] * 5,
        out_specs=vmem,
        scratch_shapes=scratch,
        compiler_params=pltpu.CompilerParams(
            collective_id=0, has_side_effects=True, vmem_limit_bytes=67043328
        ),
        name="layer",
    )(tokens, *ws, cv, cgate, co, *gains, ck, cln.reshape(1, -1))
    return res


def solution(mesh):
    fs, tp = mesh.shape["fs"], mesh.shape["tp"]
    both = P("fs", "tp")
    down = P("tp", "fs")
    in_specs = (both, P(), both, both, down, P(), both, both, P(None, "tp"), P("tp"), down, P(), both, both, down)
    return jax.shard_map(
        partial(per_device, fs, tp), mesh=mesh, in_specs=in_specs, out_specs=both, check_vma=False
    )
```
